256 devices in a mesh: sp: 64 (over z, x, core), tp: 4 (over y).
Axes of the slice: x: 4, y: 4, z: 8, core: 2. Of those that a mesh axis runs over, the one named last changes fastest.
Arguments:
- residual_in: bfloat16 [16384, 2048], P(('sp', 'tp')), may hold values from -0.119628906 to 0.119628906
- queries: bfloat16 [16384, 2048], P('sp', 'tp'), may hold values from -6 to 6
- keys_raw: bfloat16 [16384, 512], P('sp', 'tp'), may hold values from -6 to 6
- values_raw: bfloat16 [16384, 512], P('sp', 'tp'), may hold values from -6 to 6
- query_gain: float32 [128], replicated, may hold values from 0.28 to 7
- key_gain: float32 [128], replicated, may hold values from 0.28 to 7
- out_weight: bfloat16 [2048, 2048], P('tp'), may hold values from -0.125 to 0.125
- norm_gain: float32 [2048], replicated, may hold values from 0.1 to 1.9
- gate_weight: bfloat16 [2048, 5632], P('sp', 'tp'), may hold values from -0.125 to 0.125
- up_weight: bfloat16 [2048, 5632], P('sp', 'tp'), may hold values from -0.125 to 0.125
- down_weight: bfloat16 [5632, 2048], P('tp', 'sp'), may hold values from -0.078125 to 0.078125
Outputs:
- residual_out: bfloat16 [16384, 2048], P(('sp', 'tp'))
The draws below stay inside these ranges and needn't reach their ends.
All inputs are finite; a program needn't handle non-finite values.
Results may differ from the reference program's by a relative error of at most 0.024.
The reference program's roundings to bfloat16 on the way count: a program that leaves them out, or rounds other values in their place, can miss the bound.
Values may be sent and summed in bfloat16 or wider, within the bound.
A program may use at most 128 MiB of HBM per device.

```python
import math
import jax
import jax.numpy as jnp
from jax import lax

D = 2048
H = 16
KVH = 4
HD = 128
FF = 5632
GRID_W = 64
TOKENS = 16384
N_TP = 4


def paired_rows(key):
    keys_part = jnp.clip(jax.random.normal(jax.random.fold_in(key, 11), (TOKENS, KVH * HD), jnp.float32), -6.0, 6.0)
    query_part = jnp.clip(jax.random.normal(jax.random.fold_in(key, 12), (TOKENS, H * HD), jnp.float32), -6.0, 6.0)
    return (query_part, keys_part)


def draw_queries(key, part):
    return paired_rows(key)[0].astype(jnp.bfloat16)


def draw_keys_raw(key, part):
    return paired_rows(key)[1].astype(jnp.bfloat16)


def gain_draw(key):
    return 1.0 + 0.18 * jnp.clip(jax.random.normal(key, (HD,), jnp.float32), -4.0, 4.0)


def draw_query_gain(key, part):
    return gain_draw(jax.random.fold_in(key, 21))


def draw_key_gain(key, part):
    return gain_draw(jax.random.fold_in(key, 22))


def levels(own_key, dims, pieces, smallest, high):
    def one(dim, shards_of):
        draws = jax.random.uniform(jax.random.fold_in(jax.random.fold_in(own_key, 6), dim), (shards_of,), jnp.float32, smallest / len(pieces), high / len(pieces))
        return jnp.repeat(jnp.exp(draws), dims[dim] // shards_of).reshape((-1,) + (1,) * (len(dims) - dim - 1))

    level = one(*pieces[0])
    for cut in pieces[1:]:
        level = level * one(*cut)
    return level


def gaussian(key, extent, spread, limit, pieces=(), held_as=jnp.bfloat16):
    result = jax.random.normal(key, extent, jnp.float32) * spread
    if len(pieces) > 0:
        result = levels(key, extent, pieces, -0.22, 0.18) * result
    return jnp.clip(result, min=-limit, max=limit).astype(held_as)


def setup_inputs(seed: int = 0) -> dict:
    key_of = jax.random.split(jax.random.key(seed), 12)
    residual_in = gaussian(key_of[0], (TOKENS, D), 0.02, 0.119628906, ((0, 256),))
    queries = draw_queries(jax.random.fold_in(key_of[11], 71), 0)
    keys_raw = draw_keys_raw(jax.random.fold_in(key_of[11], 71), 0)
    values_raw = gaussian(key_of[3], (TOKENS, KVH * HD), 1.0, 6.0, ((0, 64), (1, 4)))
    query_gain = draw_query_gain(jax.random.fold_in(key_of[11], 71), 0)
    key_gain = draw_key_gain(jax.random.fold_in(key_of[11], 71), 0)
    out_weight = gaussian(key_of[6], (H * HD, D), (H * HD) ** -0.5, 0.125, ((0, 4),))
    norm_gain = jnp.clip(1.0 + 0.18 * jax.random.normal(key_of[7], (D,), jnp.float32), 0.1, 1.9)
    gate_weight = gaussian(key_of[8], (D, FF), D ** -0.5, 0.125, ((0, 64), (1, 4)))
    up_weight = gaussian(key_of[9], (D, FF), D ** -0.5, 0.125, ((0, 64), (1, 4)))
    down_weight = gaussian(key_of[10], (FF, D), FF ** -0.5, 0.078125, ((0, 4), (1, 64)))
    return {"residual_in": residual_in, "queries": queries, "keys_raw": keys_raw, "values_raw": values_raw, "query_gain": query_gain, "key_gain": key_gain, "out_weight": out_weight, "norm_gain": norm_gain, "gate_weight": gate_weight, "up_weight": up_weight, "down_weight": down_weight}


EPS = 1e-06
THETA = 10000.0

def turn_half(part, angles):
    quarter = part.shape[-1] // 2
    cosine = jnp.cos(angles)[:, None, :]
    sine = jnp.sin(angles)[:, None, :]
    first = part[..., :quarter]
    second = part[..., quarter:]
    return part * cosine + jnp.concatenate([-second, first], axis=-1) * sine

def prepare_heads(raw, gain, positions, heads):
    count = raw.shape[0]
    head_dim = gain.shape[0]
    half = head_dim // 2
    vec = raw.astype(jnp.float32).reshape(count, heads, head_dim)
    vec = vec * lax.rsqrt(lax.optimization_barrier(jnp.mean(vec * vec, axis=-1, keepdims=True)) + EPS) * gain
    freqs = THETA ** (-jnp.arange(0, half, 2, dtype=jnp.float32) / half)
    row_ang = (positions // GRID_W).astype(jnp.float32)[:, None] * freqs
    col_ang = (positions % GRID_W).astype(jnp.float32)[:, None] * freqs
    row_ang = jnp.concatenate([row_ang, row_ang], axis=-1)
    col_ang = jnp.concatenate([col_ang, col_ang], axis=-1)
    turned = jnp.concatenate([turn_half(vec[..., :half], row_ang), turn_half(vec[..., half:], col_ang)], axis=-1)
    return turned.astype(jnp.bfloat16)

def reference(residual_in, queries, keys_raw, values_raw, query_gain, key_gain, out_weight, norm_gain, gate_weight, up_weight, down_weight):
    positions = jnp.arange(TOKENS, dtype=jnp.int32)
    group = H // KVH
    q_rot = prepare_heads(queries, query_gain, positions, H)
    k_rot = prepare_heads(keys_raw, key_gain, positions, KVH).astype(jnp.float32)
    vals = values_raw.reshape(TOKENS, KVH, HD).astype(jnp.float32)
    block = math.gcd(TOKENS, 256)
    q_blocks = q_rot.reshape(TOKENS // block, block, KVH, group, HD)

    def attend(q_blk):
        scores = jnp.einsum('qkgd,skd->qkgs', q_blk.astype(jnp.float32), k_rot) * HD ** (-0.5)
        top = lax.optimization_barrier(jnp.max(scores, axis=-1, keepdims=True))
        expo = jnp.exp(scores - top)
        total = lax.optimization_barrier(jnp.sum(expo, axis=-1))
        rounded = lax.optimization_barrier(expo.astype(jnp.bfloat16)).astype(jnp.float32)
        summed = jnp.einsum('qkgs,skd->qkgd', rounded, vals)
        return (summed / total[..., None]).astype(jnp.bfloat16)
    attended = lax.map(attend, q_blocks).reshape(TOKENS, H * HD)
    head_cols = H * HD // N_TP
    projected = jnp.zeros((TOKENS, D), jnp.float32)
    for grp in range(N_TP):
        term = jnp.dot(attended[:, grp * head_cols:(grp + 1) * head_cols], out_weight[grp * head_cols:(grp + 1) * head_cols], preferred_element_type=jnp.float32)
        projected = projected + lax.optimization_barrier(term.astype(jnp.bfloat16)).astype(jnp.float32)
    mixed = (residual_in.astype(jnp.float32) + projected).astype(jnp.bfloat16)
    mixed_f = mixed.astype(jnp.float32)
    normed = (mixed_f * lax.rsqrt(lax.optimization_barrier(jnp.mean(mixed_f * mixed_f, axis=-1, keepdims=True)) + EPS) * norm_gain).astype(jnp.bfloat16)
    gate = jnp.dot(normed, gate_weight, preferred_element_type=jnp.float32)
    up_val = jnp.dot(normed, up_weight, preferred_element_type=jnp.float32)
    hidden = (jax.nn.silu(gate) * up_val).astype(jnp.bfloat16)
    unit_rows = FF // N_TP
    fed = jnp.zeros((TOKENS, D), jnp.float32)
    for grp in range(N_TP):
        term = jnp.dot(hidden[:, grp * unit_rows:(grp + 1) * unit_rows], down_weight[grp * unit_rows:(grp + 1) * unit_rows], preferred_element_type=jnp.float32)
        fed = fed + lax.optimization_barrier(term.astype(jnp.bfloat16)).astype(jnp.float32)
    return (mixed_f + 0.5 * fed).astype(jnp.bfloat16)
```

```python
import functools
import math

import jax
import jax.numpy as jnp
import numpy as np
from jax import lax
from jax.experimental import pallas as pl
from jax.experimental.pallas import tpu as pltpu
from jax.sharding import PartitionSpec as P

GRID_W = 64
EPS = 1e-06
THETA = 10000.0
MESH = pl.DeviceIdType.MESH
NZ, NX = 8, 4
F32 = jnp.float32
BF16 = jnp.bfloat16


def next_hops(color, dz, dx):
    out = []
    if color == 0:
        if dx == 0:
            if 0 <= dz < 4:
                out.append(("z+", dz + 1, 0))
            if -3 < dz <= 0:
                out.append(("z-", dz - 1, 0))
            out.append(("x+", dz, 1))
            out.append(("x-", dz, -1))
        elif dx == 1 and dz % 2 == 0:
            out.append(("x+", dz, 2))
        elif dx == -1 and dz % 2 == 1:
            out.append(("x-", dz, -2))
    else:
        if dz == 0:
            if dx == 0:
                out.append(("x+", 0, 1))
                out.append(("x-", 0, -1))
            elif dx == 1:
                out.append(("x+", 0, 2))
            out.append(("z+", 1, dx))
            out.append(("z-", -1, dx))
        elif dz > 0:
            if dz < (4 if dx % 2 == 0 else 3):
                out.append(("z+", dz + 1, dx))
        else:
            if -dz < (3 if dx % 2 == 0 else 4):
                out.append(("z-", dz - 1, dx))
    return out


def blocks_of(color):
    seen, todo = [], [(0, 0)]
    while todo:
        at = todo.pop(0)
        seen.append(at)
        todo += [(dz, dx) for _, dz, dx in next_hops(color, *at)]
    assert len(seen) == NZ * NX and len({(dz % NZ, dx % NX) for dz, dx in seen}) == NZ * NX
    return seen


def slot_order():
    both = [(abs(dz) + abs(dx), i, color, dz, dx) for color in (0, 1) for i, (dz, dx) in enumerate(blocks_of(color))]
    return [(color, dz, dx) for _, _, color, dz, dx in sorted(both)]


SLOTS = slot_order()
SLOT_OF = {b: i for i, b in enumerate(SLOTS)}
N_SLOTS = len(SLOTS)
PER = 8


def rope(v, gain, cos, sin, lane):
    v = v * lax.rsqrt(jnp.mean(v * v, axis=-1, keepdims=True) + EPS) * gain
    turned = jnp.where(lane % 64 < 32, -pltpu.roll(v, 96, 1), pltpu.roll(v, 32, 1))
    return (v * cos + turned * sin).astype(BF16)


def attention_kernel(
    q_ref, k_ref, v_ref, qg_ref, kg_ref, freq_ref, out_ref,
    kv, qall, acc, top, far_acc, far_top, cos_ref, sin_ref,
    kv_recv, kv_send, swap_recv, swap_send,
):
    me = lax.axis_index("sp")
    core = me % 2
    chip = me // 2
    x = chip % NX
    z = chip // NX
    at = {
        "z+": (((z + 1) % NZ) * NX + x) * 2 + core,
        "z-": (((z + NZ - 1) % NZ) * NX + x) * 2 + core,
        "x+": (z * NX + (x + 1) % NX) * 2 + core,
        "x-": (z * NX + (x + NX - 1) % NX) * 2 + core,
    }
    partner = chip * 2 + 1 - core
    barrier = pltpu.get_barrier_semaphore()
    for dev in (*at.values(), partner):
        pl.semaphore_signal(barrier, inc=1, device_id={"sp": dev}, device_id_type=MESH)

    tok = q_ref.shape[0]
    scale = math.log2(math.e) / math.sqrt(128)
    lane = lax.broadcasted_iota(jnp.int32, (tok, 128), 1)
    token = lax.broadcasted_iota(jnp.int32, (tok, 128), 0) + me * tok
    place = jnp.where(lane < 64, token // GRID_W, token % GRID_W).astype(F32)
    angle = place * freq_ref[...]
    cos_ref[...] = jnp.cos(angle)
    sin_ref[...] = jnp.sin(angle)
    k_rot = rope(k_ref[...].astype(F32), kg_ref[...], cos_ref[...], sin_ref[...], lane)
    for half in (0, 1):
        kv[half, :, 0:128] = k_rot[half * 128 : (half + 1) * 128]
        kv[half, :, 128:256] = v_ref[half * 128 : (half + 1) * 128, :]
    pl.semaphore_wait(barrier, 5)

    def send_on(slot):
        color, dz, dx = SLOTS[slot]
        for link, dz2, dx2 in next_hops(color, dz, dx):
            to = SLOT_OF[(color, dz2, dx2)]
            pltpu.make_async_remote_copy(
                kv.at[slot], kv.at[to], kv_send, kv_recv.at[to],
                device_id={"sp": at[link]}, device_id_type=MESH,
            ).start()

    def arrived(slot):
        pltpu.make_async_remote_copy(
            kv.at[slot], kv.at[slot], kv_send, kv_recv.at[slot],
            device_id={"sp": partner}, device_id_type=MESH,
        ).wait_recv()

    send_on(0)
    send_on(1)

    heads = q_ref.shape[1] // 128
    rows = heads * tok
    for h in range(heads):
        q_rot = rope(
            q_ref[:, h * 128 : (h + 1) * 128].astype(F32), qg_ref[...], cos_ref[...], sin_ref[...], lane
        )
        qall[rows + h * tok : rows + (h + 1) * tok, :] = q_rot
    swap_q = pltpu.make_async_remote_copy(
        qall.at[pl.ds(rows, rows)], qall.at[pl.ds(0, rows)], swap_send.at[0], swap_recv.at[0],
        device_id={"sp": partner}, device_id_type=MESH,
    )
    swap_q.start()
    acc[...] = jnp.zeros_like(acc)
    top[...] = jnp.full_like(top, -1e30)
    for slot in range(2, PER):
        arrived(slot)
        send_on(slot)
    swap_q.wait_recv()

    swap_acc = pltpu.make_async_remote_copy(
        acc.at[pl.ds(0, rows)], far_acc, swap_send.at[1], swap_recv.at[1],
        device_id={"sp": partner}, device_id_type=MESH,
    )
    swap_top = pltpu.make_async_remote_copy(
        top.at[pl.ds(0, rows)], far_top, swap_send.at[2], swap_recv.at[2],
        device_id={"sp": partner}, device_id_type=MESH,
    )
    ones = jnp.ones((PER * 128, 128), BF16)

    def half_step(half, _):
        for k in range(2 * (N_SLOTS // PER - 1)):

            @pl.when(half == k)
            def _():
                first = PER * (k // 2 + 1) + (k % 2) * (PER // 2)
                for slot in range(first, first + PER // 2):
                    arrived(slot)
                    send_on(slot)

        @pl.when(half == 2 * (N_SLOTS // PER) - 1)
        def _():
            swap_acc.start()
            swap_top.start()

        first = (half // 2) * PER
        keys = kv[pl.ds(first, PER), :, 0:128].reshape(PER * 128, 128)
        vals = kv[pl.ds(first, PER), :, 128:256].reshape(PER * 128, 128)
        wide = jnp.concatenate([vals, ones], axis=1)

        def block(i, _):
            r = pl.ds(pl.multiple_of((half % 2) * rows + i * tok, tok), tok)
            s = lax.dot_general(qall[r, :], keys, (((1,), (1,)), ((), ())), preferred_element_type=F32)
            old = top[r, :]
            new = jnp.maximum(old, jnp.max(s, axis=1, keepdims=True))
            top[r, :] = new
            shrink = jnp.exp2((old - new) * scale)
            w = jnp.exp2(s * scale - new[:, 0:1] * scale).astype(BF16)
            o = jnp.dot(w, wide, preferred_element_type=F32)
            acc[r, 0:128] = acc[r, 0:128] * shrink + o[:, 0:128]
            acc[r, 128:256] = acc[r, 128:256] * shrink + o[:, 128:256]
            return 0

        lax.fori_loop(0, heads, block, 0)
        return 0

    lax.fori_loop(0, 2 * (N_SLOTS // PER), half_step, 0)
    swap_acc.wait_recv()
    swap_top.wait_recv()
    for h in range(heads):
        mine = pl.ds(rows + h * tok, tok)
        far = pl.ds(h * tok, tok)
        t1, t2 = top[mine, :], far_top[far, :]
        t = jnp.maximum(t1, t2)
        a1, a2 = jnp.exp2((t1 - t) * scale), jnp.exp2((t2 - t) * scale)
        num = acc[mine, 0:128] * a1 + far_acc[far, 0:128] * a2
        den = acc[mine, 128:256] * a1 + far_acc[far, 128:256] * a2
        out_ref[:, h * 128 : (h + 1) * 128] = (num / den).astype(BF16)
    sent = kv.at[pl.ds(0, N_SLOTS - 2)]
    pltpu.make_async_remote_copy(
        sent, sent, kv_send, kv_recv.at[0], device_id={"sp": partner}, device_id_type=MESH
    ).wait_send()
    swap_q.wait_send()
    swap_acc.wait_send()
    swap_top.wait_send()


def attention(queries, keys_raw, values_raw, query_gain, key_gain):
    tok, width = queries.shape
    rows = tok * width // 128
    freq = (THETA ** (-np.arange(0, 64, 2, dtype=np.float64) / 64)).astype(np.float32)
    freq = jnp.asarray(np.tile(freq, 4)[None])
    vmem = pl.BlockSpec(memory_space=pltpu.VMEM)
    return pl.pallas_call(
        attention_kernel,
        out_shape=jax.ShapeDtypeStruct((tok, width), BF16),
        in_specs=[vmem] * 6,
        out_specs=vmem,
        scratch_shapes=[
            pltpu.VMEM((N_SLOTS, 128, 256), BF16),
            pltpu.VMEM((2 * rows, 128), BF16),
            pltpu.VMEM((2 * rows, 256), F32),
            pltpu.VMEM((2 * rows, 128), F32),
            pltpu.VMEM((rows, 256), F32),
            pltpu.VMEM((rows, 128), F32),
            pltpu.VMEM((tok, 128), F32),
            pltpu.VMEM((tok, 128), F32),
            pltpu.SemaphoreType.DMA((N_SLOTS,)),
            pltpu.SemaphoreType.DMA,
            pltpu.SemaphoreType.DMA((3,)),
            pltpu.SemaphoreType.DMA((3,)),
        ],
        compiler_params=pltpu.CompilerParams(
            collective_id=0, has_side_effects=True, vmem_limit_bytes=40 * 2**20
        ),
        cost_estimate=pl.CostEstimate(flops=9 * 10**9, bytes_accessed=2**22, transcendentals=2**24),
    )(queries, keys_raw, values_raw, query_gain[None], key_gain[None], freq)


def in_blocks(x, dim, length):
    shape = x.shape
    pieces = x.reshape(*shape[:dim], length, shape[dim] // length, *shape[dim + 1 :])
    return jnp.moveaxis(pieces, dim, 0)


def sent_and_summed(x, axis, dim):
    length = lax.axis_size(axis)
    pieces = lax.all_to_all(in_blocks(x, dim, length), axis, 0, 0, tiled=True)
    return jnp.sum(pieces.astype(jnp.float32), axis=0)


def gathered_copies(x, axis):
    length = lax.axis_size(axis)
    pieces = lax.all_to_all(jnp.broadcast_to(x[None], (length, *x.shape)), axis, 0, 0, tiled=True)
    return pieces.reshape(length * x.shape[0], x.shape[1])


def per_device(
    residual_in,
    queries,
    keys_raw,
    values_raw,
    query_gain,
    key_gain,
    out_weight,
    norm_gain,
    gate_weight,
    up_weight,
    down_weight,
):
    units = gate_weight.shape[1]
    weights = jnp.concatenate([gate_weight, up_weight, down_weight.T], axis=1)
    weights = lax.all_gather(weights, "sp", axis=0, tiled=True)
    attended = attention(queries, keys_raw, values_raw, query_gain, key_gain)
    projected = sent_and_summed(
        jnp.dot(attended, out_weight, preferred_element_type=jnp.float32).astype(jnp.bfloat16),
        "tp",
        0,
    )
    mixed = (residual_in.astype(jnp.float32) + projected).astype(jnp.bfloat16)
    mixed_f = mixed.astype(jnp.float32)
    normed = (
        mixed_f * lax.rsqrt(jnp.mean(mixed_f * mixed_f, axis=-1, keepdims=True) + EPS) * norm_gain
    ).astype(jnp.bfloat16)
    whole_rows = gathered_copies(normed, "tp")
    gate = jnp.dot(whole_rows, weights[:, :units], preferred_element_type=jnp.float32)
    up_val = jnp.dot(whole_rows, weights[:, units : 2 * units], preferred_element_type=jnp.float32)
    hidden = (jax.nn.silu(gate) * up_val).astype(jnp.bfloat16)
    terms = lax.dot_general(
        hidden, weights[:, 2 * units :], (((1,), (1,)), ((), ())), preferred_element_type=jnp.float32
    )
    fed = sent_and_summed(terms.astype(jnp.bfloat16), "tp", 0)
    return (mixed_f + 0.5 * fed).astype(jnp.bfloat16)


def solution(mesh):
    placed = (
        P(("sp", "tp"), None),
        P("sp", "tp"),
        P("sp", "tp"),
        P("sp", "tp"),
        P(),
        P(),
        P("tp", None),
        P(),
        P("sp", "tp"),
        P("sp", "tp"),
        P("tp", "sp"),
    )
    return jax.shard_map(
        per_device, mesh=mesh, in_specs=placed, out_specs=P(("sp", "tp"), None), check_vma=False
    )
```

```python
import math

import jax
import jax.numpy as jnp
import numpy as np
from jax import lax
from jax.experimental import pallas as pl
from jax.experimental.pallas import tpu as pltpu
from jax.sharding import PartitionSpec as P

GRID_W = 64
EPS = 1e-06
THETA = 10000.0
MESH = pl.DeviceIdType.MESH
NZ, NX = 8, 4
F32 = jnp.float32
BF16 = jnp.bfloat16


def next_hops(color, dz, dx):
    out = []
    if color == 0:
        if dx == 0:
            if 0 <= dz < 4:
                out.append(("z+", dz + 1, 0))
            if -3 < dz <= 0:
                out.append(("z-", dz - 1, 0))
            out.append(("x+", dz, 1))
            out.append(("x-", dz, -1))
        elif dx == 1 and dz % 2 == 0:
            out.append(("x+", dz, 2))
        elif dx == -1 and dz % 2 == 1:
            out.append(("x-", dz, -2))
    else:
        if dz == 0:
            if dx == 0:
                out.append(("x+", 0, 1))
                out.append(("x-", 0, -1))
            elif dx == 1:
                out.append(("x+", 0, 2))
            out.append(("z+", 1, dx))
            out.append(("z-", -1, dx))
        elif dz > 0:
            if dz < (4 if dx % 2 == 0 else 3):
                out.append(("z+", dz + 1, dx))
        else:
            if -dz < (3 if dx % 2 == 0 else 4):
                out.append(("z-", dz - 1, dx))
    return out


def blocks_of(color):
    seen, todo = [], [(0, 0)]
    while todo:
        at = todo.pop(0)
        seen.append(at)
        todo += [(dz, dx) for _, dz, dx in next_hops(color, *at)]
    assert len(seen) == NZ * NX and len({(dz % NZ, dx % NX) for dz, dx in seen}) == NZ * NX
    return seen


def slot_order():
    both = [(abs(dz) + abs(dx), i, color, dz, dx) for color in (0, 1) for i, (dz, dx) in enumerate(blocks_of(color))]
    return [(color, dz, dx) for _, _, color, dz, dx in sorted(both)]


SLOTS = slot_order()
SLOT_OF = {b: i for i, b in enumerate(SLOTS)}
N_SLOTS = len(SLOTS)
PER = 8
BLOCK = 128


def rope(v, gain, cos, sin, lane):
    v = v * lax.rsqrt(jnp.mean(v * v, axis=-1, keepdims=True) + EPS) * gain
    turned = jnp.where(lane % 64 < 32, -pltpu.roll(v, 96, 1), pltpu.roll(v, 32, 1))
    return (v * cos + turned * sin).astype(BF16)


def half(k):
    return pl.ds(k * 1024, 1024)


def layer_kernel(
    res_in, q_in, k_in, v_in, qg_in, kg_in, wo_in, ng_in, gate_in, up_in, down_in, freq_in, out_ref,
    kv, qall, acc, top, far_acc, far_top, cos_ref, sin_ref,
    res_ref, q_ref, k_ref, qg_ref, kg_ref, wo_ref, ng_ref, freq_ref,
    wbuf, att, terms, sums, parts, rows_ref, hidden,
    in_sem, kv_recv, kv_send, swap_recv, swap_send,
    w_recv, w_send, d2d_recv, d2d_send, rs_recv, rs_send, ag_recv, ag_send,
):
    me = lax.axis_index("sp")
    y = lax.axis_index("tp")
    core = me % 2
    chip = me // 2
    x = chip % NX
    z = chip // NX
    zs = {d: (z + NZ - d) % NZ for d in range(-4, 5)}
    xs = {d: (x + NX - d) % NX for d in range(-2, 3)}
    at = {
        "z+": (zs[-1] * NX + x) * 2 + core,
        "z-": (zs[1] * NX + x) * 2 + core,
        "x+": (z * NX + xs[-1]) * 2 + core,
        "x-": (z * NX + xs[1]) * 2 + core,
    }
    partner = chip * 2 + 1 - core
    y_up, y_down = (y + 1) % 4, (y + 3) % 4
    barrier = pltpu.get_barrier_semaphore()
    for dev in (*at.values(), partner):
        pl.semaphore_signal(barrier, inc=1, device_id={"sp": dev}, device_id_type=MESH)
    for dev in (y_up, y_down):
        pl.semaphore_signal(barrier, inc=1, device_id={"tp": dev}, device_id_type=MESH)

    pairs = [(freq_in, freq_ref), (k_in, k_ref), (kg_in, kg_ref)]
    pairs += [(v_in.at[pl.ds(h * 128, 128)], kv.at[h, :, pl.ds(128, 128)]) for h in (0, 1)]
    pairs += [(q_in, q_ref), (qg_in, qg_ref)]
    pairs += [(w, wbuf.at[2 * (NZ * NX * m + z * NX + x) + core]) for m, w in enumerate((gate_in, up_in, down_in))]
    pairs += [(wo_in, wo_ref), (res_in, res_ref), (ng_in, ng_ref)]
    loads = [pltpu.make_async_copy(a, b, in_sem.at[i]) for i, (a, b) in enumerate(pairs)]
    for load in loads:
        load.start()

    tok = q_ref.shape[0]
    heads = q_ref.shape[1] // 128
    rows = heads * tok
    scale = math.log2(math.e) / math.sqrt(128)
    lane = lax.broadcasted_iota(jnp.int32, (tok, 128), 1)
    token = lax.broadcasted_iota(jnp.int32, (tok, 128), 0) + me * tok
    place = jnp.where(lane < 64, token // GRID_W, token % GRID_W).astype(F32)
    for load in loads[:5]:
        load.wait()
    angle = place * freq_ref[...]
    cos_ref[...] = jnp.cos(angle)
    sin_ref[...] = jnp.sin(angle)
    k_rot = rope(k_ref[...].astype(F32), kg_ref[...], cos_ref[...], sin_ref[...], lane)
    for h in (0, 1):
        kv[h, :, 0:128] = k_rot[h * 128 : (h + 1) * 128]
    pl.semaphore_wait(barrier, 7)

    def send_on(slot):
        color, dz, dx = SLOTS[slot]
        for link, dz2, dx2 in next_hops(color, dz, dx):
            to = SLOT_OF[(color, dz2, dx2)]
            pltpu.make_async_remote_copy(
                kv.at[slot], kv.at[to], kv_send, kv_recv.at[to],
                device_id={"sp": at[link]}, device_id_type=MESH,
            ).start()

    def arrived(slot):
        pltpu.make_async_remote_copy(
            kv.at[slot], kv.at[slot], kv_send, kv_recv.at[slot],
            device_id={"sp": partner}, device_id_type=MESH,
        ).wait_recv()

    send_on(0)
    send_on(1)
    for load in loads[5:7]:
        load.wait()
    for h in range(heads):
        q_rot = rope(
            q_ref[:, h * 128 : (h + 1) * 128].astype(F32), qg_ref[...], cos_ref[...], sin_ref[...], lane
        )
        qall[rows + h * tok : rows + (h + 1) * tok, :] = q_rot

    def to_partner(src, dst, i):
        return pltpu.make_async_remote_copy(
            src, dst, swap_send.at[i], swap_recv.at[i], device_id={"sp": partner}, device_id_type=MESH
        )

    swap_q = to_partner(qall.at[pl.ds(rows, rows)], qall.at[pl.ds(0, rows)], 0)
    swap_acc = to_partner(acc.at[pl.ds(0, rows)], far_acc, 1)
    swap_top = to_partner(top.at[pl.ds(0, rows)], far_top, 2)
    swap_q.start()
    acc[...] = jnp.zeros_like(acc)
    top[...] = jnp.full_like(top, -1e30)
    for load in loads[7:]:
        load.wait()

    def weight_block(m, dz, dx):
        color = W_COLOR[m]
        block = wbuf.at[2 * (NZ * NX * m + zs[dz] * NX + xs[dx]) + core]
        n = W_INDEX[color][(dz, dx)]
        if (dz, dx) != (0, 0):
            pltpu.make_async_remote_copy(
                block, block, w_send, w_recv.at[m, n], device_id={"sp": partner}, device_id_type=MESH
            ).wait_recv()
        for link, dz2, dx2 in next_hops(color, dz, dx):
            pltpu.make_async_remote_copy(
                block, block, w_send, w_recv.at[m, W_INDEX[color][(dz2, dx2)]],
                device_id={"sp": at[link]}, device_id_type=MESH,
            ).start()
        pltpu.make_async_remote_copy(
            block, block, d2d_send, d2d_recv.at[m], device_id={"sp": partner}, device_id_type=MESH
        ).start()

    def weight_hop(ms, hop):
        for m in ms:
            for dz, dx in W_INDEX[W_COLOR[m]]:
                if abs(dz) + abs(dx) == hop:
                    weight_block(m, dz, dx)

    def attend(first, blocks):
        keys = kv[pl.ds(first, PER), :, 0:128].reshape(PER * 128, 128)
        vals = kv[pl.ds(first, PER), :, 128:256].reshape(PER * 128, 128)
        wide = jnp.concatenate([vals, jnp.ones((PER * 128, 128), BF16)], axis=1)
        for i in blocks:
            r = slice(i * BLOCK, (i + 1) * BLOCK)
            s = lax.dot_general(qall[r, :], keys, (((1,), (1,)), ((), ())), preferred_element_type=F32)
            old = top[r, :]
            new = jnp.maximum(old, jnp.max(s, axis=1, keepdims=True))
            top[r, :] = new
            shrink = jnp.exp2((old - new) * scale)
            w = jnp.exp2(s * scale - new[:, 0:1] * scale).astype(BF16)
            o = jnp.dot(w, wide, preferred_element_type=F32)
            acc[r, 0:128] = acc[r, 0:128] * shrink + o[:, 0:128]
            acc[r, 128:256] = acc[r, 128:256] * shrink + o[:, 128:256]

    def pass_on(k):
        for slot in range(max(2, PER * k), PER * (k + 1)):
            arrived(slot)
            send_on(slot)
        for ms, hop in W_AT_CHUNK.get(k, ()):
            weight_hop(ms, hop)

    def chunk(c, _):
        for k in range(1, N_SLOTS // PER - 1):

            @pl.when(c == k)
            def _():
                pass_on(k)

        attend(c * PER, range(2 * rows // BLOCK))
        return 0

    last = N_SLOTS // PER - 1
    pass_on(0)
    swap_q.wait_recv()
    lax.fori_loop(0, last, chunk, 0)
    pass_on(last)
    attend(last * PER, range(rows // BLOCK))
    swap_acc.start()
    swap_top.start()
    attend(last * PER, range(rows // BLOCK, 2 * rows // BLOCK))
    swap_acc.wait_recv()
    swap_top.wait_recv()
    for h in range(heads):
        mine = pl.ds(rows + h * tok, tok)
        far = pl.ds(h * tok, tok)
        t1, t2 = top[mine, :], far_top[far, :]
        t = jnp.maximum(t1, t2)
        a1, a2 = jnp.exp2((t1 - t) * scale), jnp.exp2((t2 - t) * scale)
        num = acc[mine, 0:128] * a1 + far_acc[far, 0:128] * a2
        den = acc[mine, 128:256] * a1 + far_acc[far, 128:256] * a2
        o = (num / den).astype(BF16)
        for j in range(4):
            att[(j + 4 - y) % 4, :, h * 128 : (h + 1) * 128] = o[j * 64 : (j + 1) * 64]

    def hop_y(src, dst, sems, i, dev):
        send, recv = sems
        return pltpu.make_async_remote_copy(
            src, dst, send.at[i], recv.at[i], device_id={"tp": dev}, device_id_type=MESH
        )

    def sum_over_tp(n, up, down, opposite):
        sems = (rs_send.at[n], rs_recv.at[n])
        t, p, s = terms.at[n], parts.at[n], sums.at[n]
        relay_up = hop_y(t.at[opposite, :, half(0)], p.at[0], sems, 0, y_up)
        relay_down = hop_y(t.at[opposite, :, half(1)], p.at[1], sems, 1, y_down)
        direct_up = hop_y(t.at[up, :, half(1)], p.at[2], sems, 2, y_up)
        direct_down = hop_y(t.at[down, :, half(0)], p.at[3], sems, 3, y_down)
        sum_up = hop_y(s.at[0], p.at[4], sems, 4, y_up)
        sum_down = hop_y(s.at[1], p.at[5], sems, 5, y_down)

        def first():
            relay_up.start()
            direct_down.start()

        def second():
            relay_down.start()
            direct_up.start()

        def third():
            relay_up.wait_recv()
            sums[n, 0] = (parts[n, 0].astype(F32) + terms[n, up, :, 0:1024].astype(F32)).astype(BF16)
            sum_up.start()
            relay_down.wait_recv()
            sums[n, 1] = (parts[n, 1].astype(F32) + terms[n, down, :, 1024:2048].astype(F32)).astype(BF16)
            sum_down.start()

        def total():
            direct_down.wait_recv()
            direct_up.wait_recv()
            sum_up.wait_recv()
            sum_down.wait_recv()
            low = terms[n, 0, :, 0:1024].astype(F32) + parts[n, 3].astype(F32) + parts[n, 4].astype(F32)
            high = terms[n, 0, :, 1024:2048].astype(F32) + parts[n, 2].astype(F32) + parts[n, 5].astype(F32)
            return jnp.concatenate([low, high], axis=1)

        def sent():
            for c in (relay_up, relay_down, direct_up, direct_down, sum_up, sum_down):
                c.wait_send()

        return first, second, third, total, sent

    first, second, third, total, sent = sum_over_tp(0, 1, 3, 2)
    lhs = att[...].reshape(tok, heads * 128)
    for k, go in ((0, first), (1, second)):
        piece = jnp.dot(lhs, wo_ref[:, k * 1024 : (k + 1) * 1024], preferred_element_type=F32)
        terms[0, :, :, k * 1024 : (k + 1) * 1024] = piece.astype(BF16).reshape(4, 64, 1024)
        go()
    for ms, hop in W_AFTER["projected"]:
        weight_hop(ms, hop)
    third()
    for ms, hop in W_AFTER["relayed"]:
        weight_hop(ms, hop)
    mixed = (res_ref[...].astype(F32) + total()).astype(BF16)
    res_ref[...] = mixed
    mixed_f = mixed.astype(F32)
    normed = mixed_f * lax.rsqrt(jnp.mean(mixed_f * mixed_f, axis=-1, keepdims=True) + EPS) * ng_ref[...]
    rows_ref[0] = normed.astype(BF16)

    ag = (ag_send, ag_recv)
    own_up = [hop_y(rows_ref.at[0, :, half(k)], rows_ref.at[1, :, half(k)], ag, k, y_up) for k in (0, 1)]
    own_down = [hop_y(rows_ref.at[0, :, half(k)], rows_ref.at[2, :, half(k)], ag, 2 + k, y_down) for k in (0, 1)]
    on_up = hop_y(rows_ref.at[1, :, half(0)], rows_ref.at[3, :, half(0)], ag, 4, y_up)
    on_down = hop_y(rows_ref.at[2, :, half(1)], rows_ref.at[3, :, half(1)], ag, 5, y_down)
    own_up[0].start()
    own_down[1].start()
    own_up[1].start()
    own_down[0].start()
    for ms, hop in W_AFTER["normed"]:
        weight_hop(ms, hop)
    own_up[0].wait_recv()
    on_up.start()
    own_down[1].wait_recv()
    on_down.start()
    for ms, hop in W_AFTER["passed"]:
        weight_hop(ms, hop)
    for c in (own_up[1], own_down[0], on_up, on_down):
        c.wait_recv()

    def from_partner(m):
        whole = wbuf.at[pl.ds(0, NZ * NX)]
        return pltpu.make_async_remote_copy(
            whole, whole, d2d_send, d2d_recv.at[m], device_id={"sp": partner}, device_id_type=MESH
        )

    from_partner(0).wait_recv()
    from_partner(1).wait_recv()
    units = hidden.shape[1]
    for n in range(units // 128):
        cols = slice(n * 128, (n + 1) * 128)
        both = jnp.concatenate(
            [wbuf[64 * m : 64 * (m + 1), :, cols].reshape(NZ * NX * 64, 128) for m in (0, 1)], axis=1
        )
        gu = jnp.dot(rows_ref[...].reshape(tok, NZ * NX * 64), both, preferred_element_type=F32)
        gate, up = gu[:, 0:128], gu[:, 128:256]
        hidden[:, cols] = (gate / (1.0 + jnp.exp(-gate)) * up).astype(BF16)
        for ms, hop in W_IN_FFN.get(n, ()):
            weight_hop(ms, hop)
    from_partner(2).wait_recv()
    first, second, third, total, sent2 = sum_over_tp(1, 2, 1, 3)
    for k in range(NZ):
        piece = lax.dot_general(
            hidden[...], wbuf[128 + 8 * k : 136 + 8 * k].reshape(256, units), (((1,), (1,)), ((), ())), preferred_element_type=F32
        )
        terms[1, :, :, k * 256 : (k + 1) * 256] = piece.astype(BF16).reshape(4, 64, 256)
        if k == NZ // 2 - 1:
            first()
    second()
    third()
    out_ref[...] = (res_ref[...].astype(F32) + 0.5 * total()).astype(BF16)

    moved = kv.at[pl.ds(0, N_SLOTS - 2)]
    pltpu.make_async_remote_copy(
        moved, moved, kv_send, kv_recv.at[0], device_id={"sp": partner}, device_id_type=MESH
    ).wait_send()
    for blocks, sem in ((3 * (NZ * NX - 1), w_send), (3 * NZ * NX, d2d_send)):
        moved = wbuf.at[pl.ds(0, blocks)]
        pltpu.make_async_remote_copy(
            moved, moved, sem, d2d_recv.at[0], device_id={"sp": partner}, device_id_type=MESH
        ).wait_send()
    for c in (swap_q, swap_acc, swap_top, *own_up, *own_down, on_up, on_down):
        c.wait_send()
    sent()
    sent2()


W_COLOR = (0, 1, 0)
W_INDEX = [{b: i for i, b in enumerate(blocks_of(color))} for color in (0, 1)]
GU, DOWN = (0, 1), (2,)
W_AT_CHUNK = {1: [(GU, 0)], 3: [(GU, 1)], 5: [(GU, 2)], 7: [(GU, 3)]}
W_AFTER = {
    "projected": [(GU, 4), (DOWN, 0)],
    "relayed": [(GU, 5), (DOWN, 1)],
    "normed": [(GU, 6), (DOWN, 2)],
    "passed": [(DOWN, 3)],
}
W_IN_FFN = {2: [(DOWN, 4)], 5: [(DOWN, 5)], 8: [(DOWN, 6)]}


def per_device(
    residual_in,
    queries,
    keys_raw,
    values_raw,
    query_gain,
    key_gain,
    out_weight,
    norm_gain,
    gate_weight,
    up_weight,
    down_weight,
):
    tok, width = queries.shape
    rows = tok * width // 128
    d = residual_in.shape[1]
    units = gate_weight.shape[1]
    freq = (THETA ** (-np.arange(0, 64, 2, dtype=np.float64) / 64)).astype(np.float32)
    freq = jnp.asarray(np.tile(freq, 4)[None])
    dma = pltpu.SemaphoreType.DMA
    return pl.pallas_call(
        layer_kernel,
        out_shape=jax.ShapeDtypeStruct(residual_in.shape, BF16),
        in_specs=[pl.BlockSpec(memory_space=pl.ANY)] * 12,
        out_specs=pl.BlockSpec(memory_space=pltpu.VMEM),
        scratch_shapes=[
            pltpu.VMEM((N_SLOTS, 128, 256), BF16),
            pltpu.VMEM((2 * rows, 128), BF16),
            pltpu.VMEM((2 * rows, 256), F32),
            pltpu.VMEM((2 * rows, 128), F32),
            pltpu.VMEM((rows, 256), F32),
            pltpu.VMEM((rows, 128), F32),
            pltpu.VMEM((tok, 128), F32),
            pltpu.VMEM((tok, 128), F32),
            pltpu.VMEM(residual_in.shape, BF16),
            pltpu.VMEM(queries.shape, BF16),
            pltpu.VMEM(keys_raw.shape, BF16),
            pltpu.VMEM((1, 128), F32),
            pltpu.VMEM((1, 128), F32),
            pltpu.VMEM(out_weight.shape, BF16),
            pltpu.VMEM((1, d), F32),
            pltpu.VMEM((1, 128), F32),
            pltpu.VMEM((3 * NZ * NX * 2, 32, units), BF16),
            pltpu.VMEM((4, tok // 4, width), BF16),
            pltpu.VMEM((2, 4, tok // 4, d), BF16),
            pltpu.VMEM((2, 2, tok // 4, d // 2), BF16),
            pltpu.VMEM((2, 6, tok // 4, d // 2), BF16),
            pltpu.VMEM((4, tok // 4, d), BF16),
            pltpu.VMEM((tok, units), BF16),
            dma((13,)),
            dma((N_SLOTS,)),
            dma,
            dma((3,)),
            dma((3,)),
            dma((3, NZ * NX)),
            dma,
            dma((3,)),
            dma,
            dma((2, 6)),
            dma((2, 6)),
            dma((6,)),
            dma((6,)),
        ],
        compiler_params=pltpu.CompilerParams(
            collective_id=0, has_side_effects=True, vmem_limit_bytes=60 * 2**20
        ),
    )(
        residual_in, queries, keys_raw, values_raw, query_gain[None], key_gain[None], out_weight,
        norm_gain[None], gate_weight, up_weight, down_weight.T, freq,
    )


def solution(mesh):
    placed = (
        P(("sp", "tp"), None),
        P("sp", "tp"),
        P("sp", "tp"),
        P("sp", "tp"),
        P(),
        P(),
        P("tp", None),
        P(),
        P("sp", "tp"),
        P("sp", "tp"),
        P("tp", "sp"),
    )
    return jax.shard_map(
        per_device, mesh=mesh, in_specs=placed, out_specs=P(("sp", "tp"), None), check_vma=False
    )
```

```python
import math

import jax
import jax.numpy as jnp
import numpy as np
from jax import lax
from jax.experimental import pallas as pl
from jax.experimental.pallas import tpu as pltpu
from jax.sharding import PartitionSpec as P

GRID_W = 64
EPS = 1e-06
THETA = 10000.0
MESH = pl.DeviceIdType.MESH
NZ, NX = 8, 4
F32 = jnp.float32
BF16 = jnp.bfloat16


MIRROR = {"z+": "z-", "z-": "z+", "x+": "x-", "x-": "x+"}


def next_hops(color, dz, dx):
    if color >= 2:
        return [(MIRROR[link], -a, -b) for link, a, b in next_hops(color - 2, -dz, -dx)]
    out = []
    if color == 0:
        if dx == 0:
            if 0 <= dz < 4:
                out.append(("z+", dz + 1, 0))
            if -3 < dz <= 0:
                out.append(("z-", dz - 1, 0))
            out.append(("x+", dz, 1))
            out.append(("x-", dz, -1))
        elif dx == 1 and dz % 2 == 0:
            out.append(("x+", dz, 2))
        elif dx == -1 and dz % 2 == 1:
            out.append(("x-", dz, -2))
    else:
        if dz == 0:
            if dx == 0:
                out.append(("x+", 0, 1))
                out.append(("x-", 0, -1))
            elif dx == 1:
                out.append(("x+", 0, 2))
            out.append(("z+", 1, dx))
            out.append(("z-", -1, dx))
        elif dz > 0:
            if dz < (4 if dx % 2 == 0 else 3):
                out.append(("z+", dz + 1, dx))
        else:
            if -dz < (3 if dx % 2 == 0 else 4):
                out.append(("z-", dz - 1, dx))
    return out


def blocks_of(color):
    seen, todo = [], [(0, 0)]
    while todo:
        at = todo.pop(0)
        seen.append(at)
        todo += [(dz, dx) for _, dz, dx in next_hops(color, *at)]
    assert len(seen) == NZ * NX and len({(dz % NZ, dx % NX) for dz, dx in seen}) == NZ * NX
    return seen


W_COLOR = (3, 2, 2)
SCHEDULE = {
    'start': [
        (3, 0, 0), (4, 0, 0),
    ],
    'chunk0': [
        (0, 0, 0), (1, 0, 0), (2, 0, 0), (3, 1, 0), (3, -1, 0), (3, 0, 1), (3, 0, -1), (4, 1, 0), (4, -1, 0),
        (5, 0, 0), (4, 0, 1), (5, 1, 0), (4, 0, -1),
    ],
    'chunk1': [
        (1, 0, 1), (1, 0, -1), (0, 1, 0), (0, -1, 0), (2, 0, 1), (2, 0, -1), (3, 2, 0), (3, -2, 0), (3, 1, 1),
        (3, 1, -1), (4, 2, 0), (4, -2, 0), (3, -1, 1), (3, -1, -1),
    ],
    'chunk2': [
        (4, 1, 1), (4, -1, 1), (3, 0, 2), (4, 1, -1), (4, -1, -1), (4, 0, 2), (1, 0, -2),
    ],
    'chunk3': [
        (5, 2, 0), (5, 3, 0), (3, 2, 1), (3, 2, -1), (3, -2, 1), (3, 3, 0), (3, -3, 0), (0, -2, 0),
        (2, 0, -2), (3, -2, -1), (0, 2, 0), (4, 3, 0), (4, -3, 0),
    ],
    'chunk4': [
        (3, 1, -2), (4, 2, 1), (4, -2, 1), (3, -1, -2), (3, 2, 2), (4, 2, -1), (4, -2, -1), (1, -1, 0),
        (3, 3, -1),
    ],
    'chunk5': [
        (3, -2, 2), (4, 1, 2), (4, -1, 2), (3, -3, -1), (3, 3, 1), (3, 4, 0), (3, -3, 1), (0, -3, 0),
        (1, -1, -1), (1, 1, 0), (4, -3, 1), (0, 3, 0),
    ],
    'chunk6': [
        (3, 3, -2), (4, 4, 0), (4, -3, -1), (3, 4, 1), (3, -3, -2), (4, 3, 1), (1, -1, 1), (2, 1, 0),
        (0, 0, 1), (3, 4, -1), (4, 3, -1),
    ],
    'chunk7': [
        (4, -2, 2), (4, 2, 2), (3, 4, 2), (0, 0, -1), (1, 1, 1), (1, 1, -1), (0, -4, 0), (2, 1, -1),
        (4, -4, 1), (1, -1, 2), (1, -2, 0), (1, 2, 0), (4, -4, -1), (2, 1, 1), (0, 0, -2), (1, 1, 2),
        (4, 3, 2), (4, -3, 2), (0, -1, 1), (1, -2, -1), (0, 1, 1), (1, -2, 1), (2, -1, 0), (1, 2, -1),
        (0, 1, -1), (1, 2, 1), (0, -1, -1), (1, 3, 0), (1, -2, -2), (2, 2, 0), (2, 1, 2), (0, -1, -2),
        (2, -1, -1), (4, 4, 2), (1, -3, 0), (0, 1, -2), (2, -1, 1),
    ],
    'chunk8': [
        (0, -2, 1), (1, 2, -2), (0, 2, 1), (1, 3, 1), (1, 3, -1),
    ],
    'att': [
        (0, 2, -1), (0, -2, -1), (2, 2, 1), (2, 2, -1),
    ],
    'own': [
        (1, -3, 1), (2, 3, 0), (0, -2, -2), (1, -3, -1), (0, 2, -2), (2, -1, 2), (1, -4, 0), (2, 2, -2),
        (0, 3, 1), (2, -2, 0), (1, 3, 2),
    ],
    'relay': [
        (0, -3, 1), (2, 3, -1), (0, 3, -1), (1, -3, 2), (0, -3, -1),
    ],
    'two': [
        (1, -4, -1), (0, 3, -2), (0, -3, -2), (2, 3, 1), (2, -2, -1), (0, 4, 1), (1, -4, 1),
    ],
    'opp': [
        (2, -3, 0), (0, 4, -1), (2, -2, 1), (1, -4, -2), (0, -4, -2),
    ],
    'ffn0': [
        (2, 3, 2),
    ],
    'ffn1': [
        (2, -2, -2),
    ],
    'ffn4': [
        (2, -4, 0), (2, -3, 1),
    ],
    'ffn5': [
        (2, -3, -1),
    ],
    'plane3': [
        (2, -4, -1), (2, -4, 1),
    ],
    'plane4': [
        (2, -3, 2),
    ],
    'plane6': [
        (2, -4, -2),
    ],
}
SLOTS = [(what - 3, dz, dx) for events in SCHEDULE.values() for what, dz, dx in events if what in (3, 4)]
SLOT_OF = {b: i for i, b in enumerate(SLOTS)}
N_SLOTS = len(SLOTS)
PER = 8
PLANES = (0, 1, -1, 2, -2, 3, -3, 4)
LAG = 3
BLOCK = 128


W_INDEX = [{b: i for i, b in enumerate(blocks_of(color))} for color in W_COLOR]


def rope(v, gain, cos, sin, lane):
    v = v * lax.rsqrt(jnp.mean(v * v, axis=-1, keepdims=True) + EPS) * gain
    turned = jnp.where(lane % 64 < 32, -pltpu.roll(v, 96, 1), pltpu.roll(v, 32, 1))
    return (v * cos + turned * sin).astype(BF16)


def layer_kernel(
    res_in, q_in, k_in, v_in, qg_in, kg_in, wo_in, ng_in, gate_in, up_in, down_in, freq_in, out_ref,
    kv, qall, acc, top, far_acc, far_top, cos_ref, sin_ref,
    res_ref, q_ref, k_ref, qg_ref, kg_ref, wo_ref, ng_ref, freq_ref,
    wbuf, att, proj, mix, rows_ref, hidden, terms, sums, parts,
    in_sem, kv_recv, kv_send, swap_recv, swap_send,
    w_recv, w_send, d2d_recv, d2d_send, ring_recv, ring_send, wo_recv, wo_send, rs_recv, rs_send,
):
    me = lax.axis_index("sp")
    y = lax.axis_index("tp")
    core = me % 2
    chip = me // 2
    x = chip % NX
    z = chip // NX
    zs = {d: (z + NZ - d) % NZ for d in range(-4, 5)}
    xs = {d: (x + NX - d) % NX for d in range(-2, 3)}
    at = {
        "z+": (zs[-1] * NX + x) * 2 + core,
        "z-": (zs[1] * NX + x) * 2 + core,
        "x+": (z * NX + xs[-1]) * 2 + core,
        "x-": (z * NX + xs[1]) * 2 + core,
    }
    partner = chip * 2 + 1 - core
    y_up, y_down, y_far = (y + 1) % 4, (y + 3) % 4, (y + 2) % 4
    barrier = pltpu.get_barrier_semaphore()
    for dev in (*at.values(), partner):
        pl.semaphore_signal(barrier, inc=1, device_id={"sp": dev}, device_id_type=MESH)
    for dev in (y_up, y_down):
        pl.semaphore_signal(barrier, inc=1, device_id={"tp": dev}, device_id_type=MESH)

    pairs = [(freq_in, freq_ref), (k_in, k_ref), (kg_in, kg_ref)]
    pairs += [(v_in.at[pl.ds(h * 128, 128)], kv.at[h, :, pl.ds(128, 128)]) for h in (0, 1)]
    pairs += [(q_in, q_ref), (qg_in, qg_ref)]
    pairs += [(res_in, res_ref.at[y])]
    pairs += [(wo_in.at[pl.ds(h * 256, 256)], wo_ref.at[0, h]) for h in (0, 1)]
    pairs += [(w, wbuf.at[2 * (NZ * NX * m + z * NX + x) + core]) for m, w in enumerate((gate_in, up_in, down_in))]
    pairs += [(ng_in, ng_ref)]
    loads = [pltpu.make_async_copy(a, b, in_sem.at[i]) for i, (a, b) in enumerate(pairs)]
    for load in loads:
        load.start()

    tok = q_ref.shape[0]
    heads = q_ref.shape[1] // 128
    rows = heads * tok
    scale = math.log2(math.e) / math.sqrt(128)
    lane = lax.broadcasted_iota(jnp.int32, (tok, 128), 1)
    token = lax.broadcasted_iota(jnp.int32, (tok, 128), 0) + me * tok
    place = jnp.where(lane < 64, token // GRID_W, token % GRID_W).astype(F32)
    for load in loads[:5]:
        load.wait()
    angle = place * freq_ref[...]
    cos_ref[...] = jnp.cos(angle)
    sin_ref[...] = jnp.sin(angle)
    k_rot = rope(k_ref[...].astype(F32), kg_ref[...], cos_ref[...], sin_ref[...], lane)
    for h in (0, 1):
        kv[h, :, 0:128] = k_rot[h * 128 : (h + 1) * 128]
    pl.semaphore_wait(barrier, 7)

    def send_on(slot):
        color, dz, dx = SLOTS[slot]
        for link, dz2, dx2 in next_hops(color, dz, dx):
            to = SLOT_OF[(color, dz2, dx2)]
            pltpu.make_async_remote_copy(
                kv.at[slot], kv.at[to], kv_send, kv_recv.at[to],
                device_id={"sp": at[link]}, device_id_type=MESH,
            ).start()

    def arrived(slot):
        pltpu.make_async_remote_copy(
            kv.at[slot], kv.at[slot], kv_send, kv_recv.at[slot],
            device_id={"sp": partner}, device_id_type=MESH,
        ).wait_recv()

    def gather_y(n, ref, own, below, above, slot_up, slot_down, far_up, far_down, piece):
        def hop(i, src, dst, k, dev):
            return pltpu.make_async_remote_copy(
                ref.at[src, *piece(k)], ref.at[dst, *piece(k)], ring_send.at[n, i], ring_recv.at[n, i],
                device_id={"tp": dev}, device_id_type=MESH,
            )

        return (
            [hop(k, own, slot_up, k, y_up) for k in (0, 1)],
            [hop(2 + k, own, slot_down, k, y_down) for k in (0, 1)],
            hop(4, below, far_up, 0, y_up),
            hop(5, above, far_down, 1, y_down),
        )

    def begin(ring):
        ups, downs, _, _ = ring
        ups[0].start()
        downs[1].start()
        ups[1].start()
        downs[0].start()

    res_ring = gather_y(0, res_ref, y, y_down, y_up, y, y, y_down, y_up, lambda k: (pl.ds(32 * k, 32),))
    wo_ring = gather_y(1, wo_ref, 0, 1, 2, 1, 2, 3, 3, lambda k: (core, pl.ds(128 * k, 128)))
    att_ring = gather_y(2, att, 0, 1, 2, 1, 2, 3, 3, lambda k: (pl.ds(128 * k, 128),))

    def wo_to_partner(slot, k):
        piece = wo_ref.at[slot, core, pl.ds(128 * k, 128)]
        pltpu.make_async_remote_copy(
            piece, piece, wo_send, wo_recv, device_id={"sp": partner}, device_id_type=MESH
        ).start()

    def pass_round(code):
        ring = (res_ring, wo_ring)[code // 2]
        if code % 2 == 0:
            ring[0][0].wait_recv()
            ring[2].start()
        else:
            ring[1][1].wait_recv()
            ring[3].start()
        if code >= 2:
            wo_to_partner(1 + code % 2, code % 2)

    send_on(0)
    send_on(1)
    for load in loads[7:10]:
        load.wait()
    begin(res_ring)
    begin(wo_ring)
    for load in loads[5:7]:
        load.wait()
    for h in range(heads):
        q_rot = rope(
            q_ref[:, h * 128 : (h + 1) * 128].astype(F32), qg_ref[...], cos_ref[...], sin_ref[...], lane
        )
        qall[rows + h * tok : rows + (h + 1) * tok, :] = q_rot

    def to_partner(src, dst, i):
        return pltpu.make_async_remote_copy(
            src, dst, swap_send.at[i], swap_recv.at[i], device_id={"sp": partner}, device_id_type=MESH
        )

    swap_q = to_partner(qall.at[pl.ds(rows, rows)], qall.at[pl.ds(0, rows)], 0)
    swap_acc = to_partner(acc.at[pl.ds(0, rows)], far_acc, 1)
    swap_top = to_partner(top.at[pl.ds(0, rows)], far_top, 2)
    swap_q.start()
    acc[...] = jnp.zeros_like(acc)
    top[...] = jnp.full_like(top, -1e30)
    for load in loads[10:]:
        load.wait()

    def weight_block(m, dz, dx):
        color = W_COLOR[m]
        block = wbuf.at[2 * (NZ * NX * m + zs[dz] * NX + xs[dx]) + core]
        n = W_INDEX[m][(dz, dx)]
        if (dz, dx) != (0, 0):
            pltpu.make_async_remote_copy(
                block, block, w_send, w_recv.at[m, n], device_id={"sp": partner}, device_id_type=MESH
            ).wait_recv()
        for link, dz2, dx2 in next_hops(color, dz, dx):
            pltpu.make_async_remote_copy(
                block, block, w_send, w_recv.at[m, W_INDEX[m][(dz2, dx2)]],
                device_id={"sp": at[link]}, device_id_type=MESH,
            ).start()
        pltpu.make_async_remote_copy(
            block, block, d2d_send, d2d_recv.at[m + (dz % NZ if m == 2 else 0)], device_id={"sp": partner}, device_id_type=MESH
        ).start()

    def events(point):
        for what, dz, dx in SCHEDULE.get(point, ()):
            if what == 5:
                pass_round(dz)
            elif what >= 3:
                slot = SLOT_OF[(what - 3, dz, dx)]
                if slot >= 2:
                    arrived(slot)
                    send_on(slot)
            else:
                weight_block(what, dz, dx)

    def attend(first, blocks):
        keys = kv[pl.ds(first, PER), :, 0:128].reshape(PER * 128, 128)
        vals = kv[pl.ds(first, PER), :, 128:256].reshape(PER * 128, 128)
        wide = jnp.concatenate([vals, jnp.ones((PER * 128, 128), BF16)], axis=1)
        for i in blocks:
            r = slice(i * BLOCK, (i + 1) * BLOCK)
            s = lax.dot_general(qall[r, :], keys, (((1,), (1,)), ((), ())), preferred_element_type=F32)
            old = top[r, :]
            new = jnp.maximum(old, jnp.max(s, axis=1, keepdims=True))
            top[r, :] = new
            shrink = jnp.exp2((old - new) * scale)
            w = jnp.exp2(s * scale - new[:, 0:1] * scale).astype(BF16)
            o = jnp.dot(w, wide, preferred_element_type=F32)
            acc[r, 0:128] = acc[r, 0:128] * shrink + o[:, 0:128]
            acc[r, 128:256] = acc[r, 128:256] * shrink + o[:, 128:256]

    def chunk(c, _):
        for k in range(1, N_SLOTS // PER - 1):

            @pl.when(c == k)
            def _():
                events(f"chunk{k}")

        attend(c * PER, range(2 * rows // BLOCK))
        return 0

    last = N_SLOTS // PER - 1
    events("chunk0")
    swap_q.wait_recv()
    lax.fori_loop(0, last, chunk, 0)
    events(f"chunk{last}")
    wo_ring[0][1].wait_recv()
    wo_to_partner(1, 1)
    wo_ring[1][0].wait_recv()
    wo_to_partner(2, 0)
    attend(last * PER, range(rows // BLOCK))
    swap_acc.start()
    swap_top.start()
    attend(last * PER, range(rows // BLOCK, 2 * rows // BLOCK))
    events(f"chunk{last + 1}")
    swap_acc.wait_recv()
    swap_top.wait_recv()
    for h in range(heads):
        mine = pl.ds(rows + h * tok, tok)
        far = pl.ds(h * tok, tok)
        t1, t2 = top[mine, :], far_top[far, :]
        t = jnp.maximum(t1, t2)
        a1, a2 = jnp.exp2((t1 - t) * scale), jnp.exp2((t2 - t) * scale)
        num = acc[mine, 0:128] * a1 + far_acc[far, 0:128] * a2
        den = acc[mine, 128:256] * a1 + far_acc[far, 128:256] * a2
        att[0, :, h * 128 : (h + 1) * 128] = (num / den).astype(BF16)

    def group_term(g):
        term = jnp.dot(att[g], wo_ref[g].reshape(2 * tok, NZ * NX * 64), preferred_element_type=F32)
        return term.astype(BF16).astype(F32)

    begin(att_ring)
    events("att")
    proj[...] = group_term(0)
    events("own")
    att_ring[0][0].wait_recv()
    att_ring[2].start()
    att_ring[1][1].wait_recv()
    att_ring[3].start()
    events("relay")
    for k, (slot, c) in enumerate(((3, wo_ring[2]), (3, wo_ring[3]))):
        c.wait_recv()
        wo_to_partner(slot, k)
    shared = wo_ref.at[pl.ds(1, 3), 1 - core]
    from_other = pltpu.make_async_remote_copy(
        shared, shared, wo_send, wo_recv, device_id={"sp": partner}, device_id_type=MESH
    )
    from_other.wait_recv()
    att_ring[0][1].wait_recv()
    proj[...] += group_term(1)
    att_ring[1][0].wait_recv()
    proj[...] += group_term(2)
    events("two")
    for c in (res_ring[0][0], res_ring[0][1], res_ring[1][0], res_ring[1][1], res_ring[2], res_ring[3]):
        if c is not res_ring[0][0] and c is not res_ring[1][1]:
            c.wait_recv()
    att_ring[2].wait_recv()
    att_ring[3].wait_recv()
    proj[...] += group_term(3)
    for j in range(4):
        r = slice(64 * j, 64 * (j + 1))
        mixed = (res_ref[j].astype(F32) + proj[r]).astype(BF16)
        mix[j] = mixed
        mixed_f = mixed.astype(F32)
        normed = mixed_f * lax.rsqrt(jnp.mean(mixed_f * mixed_f, axis=-1, keepdims=True) + EPS) * ng_ref[...]
        rows_ref[r] = normed.astype(BF16)
    events("opp")

    def from_partner(i, blocks):
        whole = wbuf.at[pl.ds(0, blocks)]
        return pltpu.make_async_remote_copy(
            whole, whole, d2d_send, d2d_recv.at[i], device_id={"sp": partner}, device_id_type=MESH
        )

    from_partner(0, NZ * NX).wait_recv()
    from_partner(1, NZ * NX).wait_recv()
    events("ffn0")
    units = hidden.shape[1]
    for n in range(units // 128):
        cols = slice(n * 128, (n + 1) * 128)
        both = jnp.concatenate(
            [wbuf[64 * m : 64 * (m + 1), :, cols].reshape(NZ * NX * 64, 128) for m in (0, 1)], axis=1
        )
        gu = jnp.dot(rows_ref[...], both, preferred_element_type=F32)
        gate, up = gu[:, 0:128], gu[:, 128:256]
        hidden[:, cols] = (gate / (1.0 + jnp.exp(-gate)) * up).astype(BF16)
        events(f"ffn{n + 1}")

    def plane_copies(i):
        def hop(n, src, dev):
            return pltpu.make_async_remote_copy(
                src, parts.at[i, n], rs_send.at[i, n], rs_recv.at[i, n],
                device_id={"tp": dev}, device_id_type=MESH,
            )

        low, high = pl.ds(0, 32), pl.ds(32, 32)
        return [
            hop(0, terms.at[i, y_far, low], y_up),
            hop(1, terms.at[i, y_far, high], y_down),
            hop(2, terms.at[i, y_up, high], y_up),
            hop(3, terms.at[i, y_down, low], y_down),
            hop(4, sums.at[i, 0], y_up),
            hop(5, sums.at[i, 1], y_down),
        ]

    copies = [plane_copies(i) for i in range(NZ)]

    def add_and_pass(i):
        copies[i][0].wait_recv()
        sums[i, 0] = (parts[i, 0].astype(F32) + terms[i, y_up, 0:32].astype(F32)).astype(BF16)
        copies[i][4].start()
        copies[i][1].wait_recv()
        sums[i, 1] = (parts[i, 1].astype(F32) + terms[i, y_down, 32:64].astype(F32)).astype(BF16)
        copies[i][5].start()

    for i, dz in enumerate(PLANES):
        from_partner(2 + dz % NZ, NX).wait_recv()
        rhs = wbuf[pl.ds(2 * NZ * NX * 2 + 8 * zs[dz], 8)].reshape(256, units)
        piece = lax.dot_general(hidden[...], rhs, (((1,), (1,)), ((), ())), preferred_element_type=F32)
        terms[i] = piece.astype(BF16).reshape(4, 64, 256)
        for c in copies[i][:4]:
            c.start()
        events(f"plane{i}")
        if i >= LAG:
            add_and_pass(i - LAG)
    for i in range(NZ - LAG, NZ):
        add_and_pass(i)
    for i, dz in enumerate(PLANES):
        for c in copies[i][2:]:
            c.wait_recv()
        cols = pl.ds(pl.multiple_of(256 * zs[dz], 256), 256)
        for h, (a, b) in enumerate(((3, 4), (2, 5))):
            r = slice(32 * h, 32 * (h + 1))
            fed = terms[i, y, r].astype(F32) + parts[i, a].astype(F32) + parts[i, b].astype(F32)
            out_ref[r, cols] = (mix[y, r, cols].astype(F32) + 0.5 * fed).astype(BF16)

    moved = kv.at[pl.ds(0, N_SLOTS - 2)]
    pltpu.make_async_remote_copy(
        moved, moved, kv_send, kv_recv.at[0], device_id={"sp": partner}, device_id_type=MESH
    ).wait_send()
    for blocks, sem in ((3 * (NZ * NX - 1), w_send), (3 * NZ * NX, d2d_send)):
        moved = wbuf.at[pl.ds(0, blocks)]
        pltpu.make_async_remote_copy(
            moved, moved, sem, d2d_recv.at[0], device_id={"sp": partner}, device_id_type=MESH
        ).wait_send()
    for ups, downs, a, b in (res_ring, wo_ring, att_ring):
        for c in (*ups, *downs, a, b):
            c.wait_send()
    for c in (swap_q, swap_acc, swap_top, from_other):
        c.wait_send()
    for plane in copies:
        for c in plane:
            c.wait_send()


def per_device(
    residual_in,
    queries,
    keys_raw,
    values_raw,
    query_gain,
    key_gain,
    out_weight,
    norm_gain,
    gate_weight,
    up_weight,
    down_weight,
):
    tok, width = queries.shape
    rows = tok * width // 128
    d = residual_in.shape[1]
    units = gate_weight.shape[1]
    freq = (THETA ** (-np.arange(0, 64, 2, dtype=np.float64) / 64)).astype(np.float32)
    freq = jnp.asarray(np.tile(freq, 4)[None])
    dma = pltpu.SemaphoreType.DMA
    return pl.pallas_call(
        layer_kernel,
        out_shape=jax.ShapeDtypeStruct(residual_in.shape, BF16),
        in_specs=[pl.BlockSpec(memory_space=pl.ANY)] * 12,
        out_specs=pl.BlockSpec(memory_space=pltpu.VMEM),
        scratch_shapes=[
            pltpu.VMEM((N_SLOTS, 128, 256), BF16),
            pltpu.VMEM((2 * rows, 128), BF16),
            pltpu.VMEM((2 * rows, 256), F32),
            pltpu.VMEM((2 * rows, 128), F32),
            pltpu.VMEM((rows, 256), F32),
            pltpu.VMEM((rows, 128), F32),
            pltpu.VMEM((tok, 128), F32),
            pltpu.VMEM((tok, 128), F32),
            pltpu.VMEM((4, tok // 4, d), BF16),
            pltpu.VMEM(queries.shape, BF16),
            pltpu.VMEM(keys_raw.shape, BF16),
            pltpu.VMEM((1, 128), F32),
            pltpu.VMEM((1, 128), F32),
            pltpu.VMEM((4, 2, 256, d), BF16),
            pltpu.VMEM((1, d), F32),
            pltpu.VMEM((1, 128), F32),
            pltpu.VMEM((3 * NZ * NX * 2, 32, units), BF16),
            pltpu.VMEM((4, tok, width), BF16),
            pltpu.VMEM((tok, d), F32),
            pltpu.VMEM((4, tok // 4, d), BF16),
            pltpu.VMEM((tok, d), BF16),
            pltpu.VMEM((tok, units), BF16),
            pltpu.VMEM((NZ, 4, tok // 4, 256), BF16),
            pltpu.VMEM((NZ, 2, tok // 8, 256), BF16),
            pltpu.VMEM((NZ, 6, tok // 8, 256), BF16),
            dma((14,)),
            dma((N_SLOTS,)),
            dma,
            dma((3,)),
            dma((3,)),
            dma((3, NZ * NX)),
            dma,
            dma((2 + NZ,)),
            dma,
            dma((3, 6)),
            dma((3, 6)),
            dma,
            dma,
            dma((NZ, 6)),
            dma((NZ, 6)),
        ],
        compiler_params=pltpu.CompilerParams(
            collective_id=0, has_side_effects=True, vmem_limit_bytes=60 * 2**20
        ),
    )(
        residual_in, queries, keys_raw, values_raw, query_gain[None], key_gain[None], out_weight,
        norm_gain[None], gate_weight, up_weight, down_weight.T, freq,
    )


def solution(mesh):
    placed = (
        P(("sp", "tp"), None),
        P("sp", "tp"),
        P("sp", "tp"),
        P("sp", "tp"),
        P(),
        P(),
        P("tp", None),
        P(),
        P("sp", "tp"),
        P("sp", "tp"),
        P("tp", "sp"),
    )
    return jax.shard_map(
        per_device, mesh=mesh, in_specs=placed, out_specs=P(("sp", "tp"), None), check_vma=False
    )
```

```python
import math

import jax
import jax.numpy as jnp
from jax import lax
from jax.experimental import pallas as pl
from jax.experimental.pallas import tpu as pltpu
from jax.sharding import PartitionSpec as P

GRID_W = 64
EPS = 1e-06
THETA = 10000.0
MESH = pl.DeviceIdType.MESH
NZ, NX = 8, 4
F32 = jnp.float32
BF16 = jnp.bfloat16


MIRROR = {"z+": "z-", "z-": "z+", "x+": "x-", "x-": "x+"}


def next_hops(color, dz, dx):
    if color >= 2:
        return [(MIRROR[link], -a, -b) for link, a, b in next_hops(color - 2, -dz, -dx)]
    out = []
    if color == 0:
        if dx == 0:
            if 0 <= dz < 4:
                out.append(("z+", dz + 1, 0))
            if -3 < dz <= 0:
                out.append(("z-", dz - 1, 0))
            out.append(("x+", dz, 1))
            out.append(("x-", dz, -1))
        elif dx == 1 and dz % 2 == 0:
            out.append(("x+", dz, 2))
        elif dx == -1 and dz % 2 == 1:
            out.append(("x-", dz, -2))
    else:
        if dz == 0:
            if dx == 0:
                out.append(("x+", 0, 1))
                out.append(("x-", 0, -1))
            elif dx == 1:
                out.append(("x+", 0, 2))
            out.append(("z+", 1, dx))
            out.append(("z-", -1, dx))
        elif dz > 0:
            if dz < (4 if dx % 2 == 0 else 3):
                out.append(("z+", dz + 1, dx))
        else:
            if -dz < (3 if dx % 2 == 0 else 4):
                out.append(("z-", dz - 1, dx))
    return out


def blocks_of(color):
    seen, todo = [], [(0, 0)]
    while todo:
        at = todo.pop(0)
        seen.append(at)
        todo += [(dz, dx) for _, dz, dx in next_hops(color, *at)]
    assert len(seen) == NZ * NX and len({(dz % NZ, dx % NX) for dz, dx in seen}) == NZ * NX
    return seen


W_COLOR = (3, 0, 2)
GU_PLANES = (0, -1, 1, -2, 2, -3, 3, 4)
DOWN_PLANES = (0, 1, -1, 2, -2, 3, -3, 4)
LAG = 6
SCHEDULE = {
    'start': [
        (3, 0, 0), (4, 0, 0),
    ],
    'chunk0': [
        (0, 0, 0), (1, 0, 0), (2, 0, 0), (3, 1, 0), (3, -1, 0), (3, 0, -1), (3, 0, 1), (4, 1, 0), (4, 0, 1),
        (5, 0, 0), (4, -1, 0), (5, 1, 0), (4, 0, -1),
    ],
    'chunk1': [
        (1, 0, -1), (0, -1, 0), (1, 0, 1), (0, 1, 0), (2, 0, 1), (2, 0, -1), (1, -1, 0), (3, 2, 0),
        (3, -2, 0), (3, 1, -1), (3, 1, 1), (4, 2, 0), (4, -1, 1), (3, -1, -1), (3, -1, 1),
    ],
    'chunk2': [
        (3, 0, 2), (4, 0, 2), (4, -1, -1), (4, 1, -1), (4, 1, 1), (4, -2, 0), (2, 0, -2),
    ],
    'chunk3': [
        (5, 2, 0), (5, 3, 0), (3, 2, -1), (3, 3, 0), (1, 0, 2), (1, -1, -1), (1, -1, 1), (3, -2, -1),
        (1, 1, 0), (0, -2, 0), (4, 3, 0), (3, -3, 0), (3, 1, -2), (3, 2, 1), (4, 1, 2),
    ],
    'chunk4': [
        (4, -2, 1), (4, -1, 2), (4, 2, -1), (4, 2, 1), (3, -2, 1), (3, 3, 1), (3, 3, -1), (3, -1, -2),
        (1, -2, 0),
    ],
    'chunk5': [
        (4, -2, -1), (3, 4, 0), (4, -3, 0), (3, -3, 1), (0, 2, 0), (1, -1, -2), (1, 1, 1), (1, 1, -1),
        (0, -3, 0), (3, 2, 2), (3, -3, -1), (4, 4, 0), (4, -3, 1), (3, -2, 2),
    ],
    'chunk6': [
        (4, 2, 2), (4, 3, -1), (4, -2, 2), (3, 3, -2), (1, 2, 0), (0, 0, -1), (1, -2, -1), (1, -2, 1),
        (3, 4, 1), (4, 3, 1), (3, 4, -1),
    ],
    'chunk7': [
        (4, -3, -1), (0, 0, 1), (1, 1, -2), (1, -3, 0), (0, 3, 0), (4, 3, 2), (0, -4, 0), (1, 2, 1),
        (3, -3, -2), (4, -4, 1), (2, 1, 0), (1, -2, 2), (1, 2, -1), (4, -3, 2), (1, 3, 0), (3, 4, 2),
        (0, -1, -1), (0, 1, -1), (2, -1, 0), (1, -3, 1), (4, -4, -1), (1, -3, -1), (0, 0, -2), (4, 4, 2),
    ],
    'chunk8': [
        (0, -2, -1), (0, 1, 1), (1, 2, 2), (1, 3, -1), (2, 1, 1), (2, 1, -1),
    ],
    'att': [
        (1, 3, 1), (1, 4, 0), (0, -1, 1), (2, -1, -1),
    ],
    'own': [
        (0, 2, -1), (2, -1, 1), (0, -1, -2), (1, -3, -2), (2, 2, 0), (2, 1, 2), (0, -3, -1), (1, 3, -2),
        (0, 1, -2), (2, -2, 0),
    ],
    'relay': [
        (0, -2, 1), (1, 4, -1), (1, 4, 1), (0, 2, 1), (2, -1, 2), (0, -2, -2), (2, 2, -1), (0, 3, -1),
    ],
    'two': [
        (2, 2, 1), (2, 3, 0), (2, -2, -1), (0, 2, -2), (2, -3, 0), (2, -2, 1),
    ],
    'opp': [
        (0, -3, 1), (2, 2, -2),
    ],
    'k1': [
        (1, 4, 2), (0, -3, -2), (0, 3, 1),
    ],
    'k2': [
        (2, 3, -1),
    ],
    'k4': [
        (0, 4, -1), (2, 3, 1), (2, -4, 0),
    ],
    'k5': [
        (2, -2, -2),
    ],
    'k6': [
        (0, 3, -2), (2, -3, 1), (0, -4, -2), (2, -3, -1),
    ],
    'k7': [
        (0, 4, 1), (2, 3, 2), (2, -4, -1),
    ],
    'plane1': [
        (2, -4, 1),
    ],
    'plane4': [
        (2, -3, 2),
    ],
    'plane5': [
        (2, -4, -2),
    ],
}
SLOTS = [(what - 3, dz, dx) for events in SCHEDULE.values() for what, dz, dx in events if what in (3, 4)]
SLOT_OF = {b: i for i, b in enumerate(SLOTS)}
N_SLOTS = len(SLOTS)
PER = 8
BLOCK = 128


W_INDEX = [{b: i for i, b in enumerate(blocks_of(color))} for color in W_COLOR]


def rope(v, gain, cos, sin, lane):
    v = v * lax.rsqrt(jnp.mean(v * v, axis=-1, keepdims=True) + EPS) * gain
    turned = jnp.where(lane % 64 < 32, -pltpu.roll(v, 96, 1), pltpu.roll(v, 32, 1))
    return (v * cos + turned * sin).astype(BF16)


def layer_kernel(
    res_in, q_in, k_in, v_in, qg_in, kg_in, wo_in, ng_in, gate_in, up_in, down_in, out_hbm,
    kv, qall, acc, top, far_acc, far_top, cos_ref, sin_ref,
    res_ref, q_ref, k_ref, qg_ref, kg_ref, wo_ref, ng_ref,
    wbuf, att, proj, mix, rows_ref, gu_ref, hidden, terms, sums, parts, out_ref,
    in_sem, out_sem, kv_recv, kv_send, swap_recv, swap_send,
    w_recv, w_send, d2d_recv, d2d_send, ring_recv, ring_send, wo_recv, wo_send, rs_recv, rs_last, rs_send,
):
    me = lax.axis_index("sp")
    y = lax.axis_index("tp")
    core = me % 2
    chip = me // 2
    x = chip % NX
    z = chip // NX
    zs = {d: (z + NZ - d) % NZ for d in range(-4, 5)}
    xs = {d: (x + NX - d) % NX for d in range(-2, 3)}
    at = {
        "z+": (zs[-1] * NX + x) * 2 + core,
        "z-": (zs[1] * NX + x) * 2 + core,
        "x+": (z * NX + xs[-1]) * 2 + core,
        "x-": (z * NX + xs[1]) * 2 + core,
    }
    partner = chip * 2 + 1 - core
    y_up, y_down, y_far = (y + 1) % 4, (y + 3) % 4, (y + 2) % 4
    barrier = pltpu.get_barrier_semaphore()
    for dev in (*at.values(), partner):
        pl.semaphore_signal(barrier, inc=1, device_id={"sp": dev}, device_id_type=MESH)
    for dev in (y_up, y_down):
        pl.semaphore_signal(barrier, inc=1, device_id={"tp": dev}, device_id_type=MESH)

    pairs = [(k_in, k_ref), (kg_in, kg_ref), (v_in, kv.at[pl.ds(0, 2), :, pl.ds(128, 128)])]
    pairs += [(q_in, q_ref), (qg_in, qg_ref)]
    pairs += [(res_in, res_ref.at[y])]
    pairs += [(wo_in, wo_ref.at[0])]
    pairs += [(w, wbuf.at[2 * (NZ * NX * m + z * NX + x) + core]) for m, w in enumerate((gate_in, up_in, down_in))]
    pairs += [(ng_in, ng_ref)]
    loads = [pltpu.make_async_copy(a, b, in_sem.at[i]) for i, (a, b) in enumerate(pairs)]
    for load in loads:
        load.start()

    tok = q_ref.shape[0]
    heads = q_ref.shape[1] // 128
    rows = heads * tok
    scale = math.log2(math.e) / math.sqrt(128)
    lane = lax.broadcasted_iota(jnp.int32, (tok, 128), 1)
    token = lax.broadcasted_iota(jnp.int32, (tok, 128), 0) + me * tok
    place = jnp.where(lane < 64, token // GRID_W, token % GRID_W).astype(F32)
    angle = place * jnp.exp2((lane % 32).astype(F32) * (-math.log2(THETA) / 32))
    cos_ref[...] = jnp.cos(angle)
    sin_ref[...] = jnp.sin(angle)
    for load in loads[:3]:
        load.wait()
    k_rot = rope(k_ref[...].astype(F32), kg_ref[...], cos_ref[...], sin_ref[...], lane)
    for h in (0, 1):
        kv[h, :, 0:128] = k_rot[h * 128 : (h + 1) * 128]
    pl.semaphore_wait(barrier, 7)

    def send_on(slot):
        color, dz, dx = SLOTS[slot]
        for link, dz2, dx2 in next_hops(color, dz, dx):
            to = SLOT_OF[(color, dz2, dx2)]
            pltpu.make_async_remote_copy(
                kv.at[slot], kv.at[to], kv_send, kv_recv.at[to],
                device_id={"sp": at[link]}, device_id_type=MESH,
            ).start()

    def arrived(slot):
        pltpu.make_async_remote_copy(
            kv.at[slot], kv.at[slot], kv_send, kv_recv.at[slot],
            device_id={"sp": partner}, device_id_type=MESH,
        ).wait_recv()

    def gather_y(n, ref, own, below, above, slot_up, slot_down, far_up, far_down, piece):
        def hop(i, src, dst, k, dev):
            return pltpu.make_async_remote_copy(
                ref.at[src, *piece(k)], ref.at[dst, *piece(k)], ring_send.at[n], ring_recv.at[n, i],
                device_id={"tp": dev}, device_id_type=MESH,
            )

        return (
            [hop(k, own, slot_up, k, y_up) for k in (0, 1)],
            [hop(2 + k, own, slot_down, k, y_down) for k in (0, 1)],
            hop(4, below, far_up, 0, y_up),
            hop(5, above, far_down, 1, y_down),
        )

    def begin(ring):
        ups, downs, _, _ = ring
        ups[0].start()
        downs[1].start()
        ups[1].start()
        downs[0].start()

    res_ring = gather_y(0, res_ref, y, y_down, y_up, y, y, y_down, y_up, lambda k: (pl.ds(32 * k, 32),))
    wo_ring = gather_y(1, wo_ref, 0, 1, 2, 1, 2, 3, 3, lambda k: (core, pl.ds(128 * k, 128)))
    att_ring = gather_y(2, att, 0, 1, 2, 1, 2, 3, 3, lambda k: (pl.ds(128 * k, 128),))

    def wo_to_partner(slot, k):
        piece = wo_ref.at[slot, core, pl.ds(128 * k, 128)]
        pltpu.make_async_remote_copy(
            piece, piece, wo_send, wo_recv, device_id={"sp": partner}, device_id_type=MESH
        ).start()

    def pass_round(code):
        ring = (res_ring, wo_ring)[code // 2]
        if code % 2 == 0:
            ring[0][0].wait_recv()
            ring[2].start()
        else:
            ring[1][1].wait_recv()
            ring[3].start()
        if code >= 2:
            wo_to_partner(1 + code % 2, code % 2)

    send_on(0)
    send_on(1)
    for load in loads[5:7]:
        load.wait()
    begin(res_ring)
    begin(wo_ring)
    for load in loads[3:5]:
        load.wait()
    for h in range(heads):
        q_rot = rope(
            q_ref[:, h * 128 : (h + 1) * 128].astype(F32), qg_ref[...], cos_ref[...], sin_ref[...], lane
        )
        qall[rows + h * tok : rows + (h + 1) * tok, :] = q_rot

    def to_partner(src, dst, i):
        return pltpu.make_async_remote_copy(
            src, dst, swap_send.at[i], swap_recv.at[i], device_id={"sp": partner}, device_id_type=MESH
        )

    swap_q = to_partner(qall.at[pl.ds(rows, rows)], qall.at[pl.ds(0, rows)], 0)
    swap_acc = to_partner(acc.at[pl.ds(0, rows)], far_acc, 1)
    swap_top = to_partner(top.at[pl.ds(0, rows)], far_top, 2)
    swap_q.start()
    acc[...] = jnp.zeros_like(acc)
    top[...] = jnp.full_like(top, -1e30)
    for load in loads[7:]:
        load.wait()

    def weight_block(m, dz, dx):
        color = W_COLOR[m]
        block = wbuf.at[2 * (NZ * NX * m + zs[dz] * NX + xs[dx]) + core]
        n = W_INDEX[m][(dz, dx)]
        if (dz, dx) != (0, 0):
            pltpu.make_async_remote_copy(
                block, block, w_send, w_recv.at[m, n], device_id={"sp": partner}, device_id_type=MESH
            ).wait_recv()
        for link, dz2, dx2 in next_hops(color, dz, dx):
            pltpu.make_async_remote_copy(
                block, block, w_send, w_recv.at[m, W_INDEX[m][(dz2, dx2)]],
                device_id={"sp": at[link]}, device_id_type=MESH,
            ).start()
        pltpu.make_async_remote_copy(
            block, block, d2d_send, d2d_recv.at[m, dz % NZ], device_id={"sp": partner}, device_id_type=MESH
        ).start()

    def events(point):
        for what, dz, dx in SCHEDULE.get(point, ()):
            if what == 5:
                pass_round(dz)
            elif what >= 3:
                slot = SLOT_OF[(what - 3, dz, dx)]
                if slot >= 2:
                    arrived(slot)
                    send_on(slot)
            else:
                weight_block(what, dz, dx)

    def attend(first, blocks):
        keys = kv[pl.ds(first, PER), :, 0:128].reshape(PER * 128, 128)
        vals = kv[pl.ds(first, PER), :, 128:256].reshape(PER * 128, 128)
        wide = jnp.concatenate([vals, jnp.ones((PER * 128, 128), BF16)], axis=1)
        for i in blocks:
            r = slice(i * BLOCK, (i + 1) * BLOCK)
            s = lax.dot_general(qall[r, :], keys, (((1,), (1,)), ((), ())), preferred_element_type=F32)
            old = top[r, :]
            new = jnp.maximum(old, jnp.max(s, axis=1, keepdims=True))
            top[r, :] = new
            shrink = jnp.exp2((old - new) * scale)
            w = jnp.exp2(s * scale - new[:, 0:1] * scale).astype(BF16)
            o = jnp.dot(w, wide, preferred_element_type=F32)
            acc[r, 0:128] = acc[r, 0:128] * shrink + o[:, 0:128]
            acc[r, 128:256] = acc[r, 128:256] * shrink + o[:, 128:256]

    def chunk(c, _):
        for k in range(1, N_SLOTS // PER - 1):

            @pl.when(c == k)
            def _():
                events(f"chunk{k}")

        attend(c * PER, range(2 * rows // BLOCK))
        return 0

    last = N_SLOTS // PER - 1
    events("chunk0")
    swap_q.wait_recv()
    lax.fori_loop(0, last, chunk, 0)
    events(f"chunk{last}")
    wo_ring[0][1].wait_recv()
    wo_to_partner(1, 1)
    wo_ring[1][0].wait_recv()
    wo_to_partner(2, 0)
    attend(last * PER, range(rows // BLOCK))
    swap_acc.start()
    swap_top.start()
    attend(last * PER, range(rows // BLOCK, 2 * rows // BLOCK))
    events(f"chunk{last + 1}")
    for k in (0, 1):
        wo_ring[2 + k].wait_recv()
        wo_to_partner(3, k)
    swap_acc.wait_recv()
    swap_top.wait_recv()
    for h in range(heads):
        mine = pl.ds(rows + h * tok, tok)
        far = pl.ds(h * tok, tok)
        t1, t2 = top[mine, :], far_top[far, :]
        t = jnp.maximum(t1, t2)
        a1, a2 = jnp.exp2((t1 - t) * scale), jnp.exp2((t2 - t) * scale)
        num = acc[mine, 0:128] * a1 + far_acc[far, 0:128] * a2
        den = acc[mine, 128:256] * a1 + far_acc[far, 128:256] * a2
        att[0, :, h * 128 : (h + 1) * 128] = (num / den).astype(BF16)

    def group_term(g):
        term = jnp.dot(att[g], wo_ref[g].reshape(2 * tok, NZ * NX * 64), preferred_element_type=F32)
        return term.astype(BF16).astype(F32)

    begin(att_ring)
    events("att")
    proj[...] = group_term(0)
    events("own")
    att_ring[0][0].wait_recv()
    att_ring[2].start()
    att_ring[1][1].wait_recv()
    att_ring[3].start()
    events("relay")
    shared = wo_ref.at[pl.ds(1, 3), 1 - core]
    from_other = pltpu.make_async_remote_copy(
        shared, shared, wo_send, wo_recv, device_id={"sp": partner}, device_id_type=MESH
    )
    from_other.wait_recv()
    att_ring[0][1].wait_recv()
    proj[...] += group_term(1)
    att_ring[1][0].wait_recv()
    proj[...] += group_term(2)
    events("two")
    for c in (res_ring[0][0], res_ring[0][1], res_ring[1][0], res_ring[1][1], res_ring[2], res_ring[3]):
        if c is not res_ring[0][0] and c is not res_ring[1][1]:
            c.wait_recv()
    att_ring[2].wait_recv()
    att_ring[3].wait_recv()
    proj[...] += group_term(3)
    for j in range(4):
        r = slice(64 * j, 64 * (j + 1))
        mixed = (res_ref[j].astype(F32) + proj[r]).astype(BF16)
        mix[j] = mixed
        mixed_f = mixed.astype(F32)
        normed = mixed_f * lax.rsqrt(jnp.mean(mixed_f * mixed_f, axis=-1, keepdims=True) + EPS) * ng_ref[...]
        rows_ref[r] = normed.astype(BF16)
    events("opp")

    def plane_of(m, dz):
        four = wbuf.at[pl.ds(0, NX)]
        pltpu.make_async_remote_copy(
            four, four, d2d_send, d2d_recv.at[m, dz % NZ], device_id={"sp": partner}, device_id_type=MESH
        ).wait_recv()
        return wbuf[pl.ds(2 * (NZ * NX * m + NX * zs[dz]), 2 * NX)].reshape(64 * NX, units)

    units = hidden.shape[1]
    for n, dz in enumerate(GU_PLANES):
        lhs = rows_ref[:, pl.ds(pl.multiple_of(256 * zs[dz], 256), 256)]
        for m in (0, 1):
            part = jnp.dot(lhs, plane_of(m, dz), preferred_element_type=F32)
            gu_ref[m] = part if n == 0 else gu_ref[m] + part
        events(f"k{n + 1}")
    gate = gu_ref[0]
    hidden[...] = (gate / (1.0 + jnp.exp(-gate)) * gu_ref[1]).astype(BF16)

    def plane_copies(i):
        def hop(n, src, dev):
            return pltpu.make_async_remote_copy(
                src, parts.at[i, n], rs_send, rs_recv.at[i, n] if n < 2 else rs_last,
                device_id={"tp": dev}, device_id_type=MESH,
            )

        low, high = pl.ds(0, 32), pl.ds(32, 32)
        return [
            hop(0, terms.at[i, y_far, low], y_up),
            hop(1, terms.at[i, y_far, high], y_down),
            hop(2, terms.at[i, y_up, high], y_up),
            hop(3, terms.at[i, y_down, low], y_down),
            hop(4, sums.at[i, 0], y_up),
            hop(5, sums.at[i, 1], y_down),
        ]

    copies = [plane_copies(i) for i in range(NZ)]

    def add_and_pass(i):
        copies[i][0].wait_recv()
        sums[i, 0] = (parts[i, 0].astype(F32) + terms[i, y_up, 0:32].astype(F32)).astype(BF16)
        copies[i][4].start()
        copies[i][1].wait_recv()
        sums[i, 1] = (parts[i, 1].astype(F32) + terms[i, y_down, 32:64].astype(F32)).astype(BF16)
        copies[i][5].start()

    for i, dz in enumerate(DOWN_PLANES):
        piece = lax.dot_general(hidden[...], plane_of(2, dz), (((1,), (1,)), ((), ())), preferred_element_type=F32)
        terms[i] = piece.astype(BF16).reshape(4, 64, 256)
        for c in copies[i][:4]:
            c.start()
        events(f"plane{i}")
        if i >= LAG:
            add_and_pass(i - LAG)
    for i in range(NZ - LAG, NZ):
        add_and_pass(i)
    last_pieces = parts.at[:, pl.ds(2, 4)]
    pltpu.make_async_remote_copy(
        last_pieces, last_pieces, rs_send, rs_last, device_id={"tp": y_up}, device_id_type=MESH
    ).wait_recv()
    for i, dz in enumerate(DOWN_PLANES):
        cols = pl.ds(pl.multiple_of(256 * zs[dz], 256), 256)
        for h, (a, b) in enumerate(((3, 4), (2, 5))):
            r = slice(32 * h, 32 * (h + 1))
            fed = terms[i, y, r].astype(F32) + parts[i, a].astype(F32) + parts[i, b].astype(F32)
            out_ref[r, cols] = (mix[y, r, cols].astype(F32) + 0.5 * fed).astype(BF16)
    out = pltpu.make_async_copy(out_ref, out_hbm, out_sem)
    out.start()
    moved = kv.at[pl.ds(0, N_SLOTS - 2)]
    pltpu.make_async_remote_copy(
        moved, moved, kv_send, kv_recv.at[0], device_id={"sp": partner}, device_id_type=MESH
    ).wait_send()
    for blocks, sem in ((3 * (NZ * NX - 1), w_send), (3 * NZ * NX, d2d_send)):
        moved = wbuf.at[pl.ds(0, blocks)]
        pltpu.make_async_remote_copy(
            moved, moved, sem, d2d_recv.at[0, 0], device_id={"sp": partner}, device_id_type=MESH
        ).wait_send()
    for n, sent in enumerate((res_ref.at[pl.ds(0, 3)], wo_ref.at[pl.ds(0, 3), 0], att.at[pl.ds(0, 3)])):
        pltpu.make_async_remote_copy(
            sent, sent, ring_send.at[n], ring_recv.at[n, 0], device_id={"tp": y_up}, device_id_type=MESH
        ).wait_send()
    for c in (swap_q, swap_acc, swap_top, from_other):
        c.wait_send()
    pltpu.make_async_remote_copy(
        parts, parts, rs_send, rs_last, device_id={"tp": y_up}, device_id_type=MESH
    ).wait_send()
    out.wait()


def per_device(
    residual_in,
    queries,
    keys_raw,
    values_raw,
    query_gain,
    key_gain,
    out_weight,
    norm_gain,
    gate_weight,
    up_weight,
    down_weight,
):
    tok, width = queries.shape
    rows = tok * width // 128
    d = residual_in.shape[1]
    units = gate_weight.shape[1]
    dma = pltpu.SemaphoreType.DMA
    return pl.pallas_call(
        layer_kernel,
        out_shape=jax.ShapeDtypeStruct(residual_in.shape, BF16),
        in_specs=[pl.BlockSpec(memory_space=pl.ANY)] * 11,
        out_specs=pl.BlockSpec(memory_space=pl.ANY),
        scratch_shapes=[
            pltpu.VMEM((N_SLOTS, 128, 256), BF16),
            pltpu.VMEM((2 * rows, 128), BF16),
            pltpu.VMEM((2 * rows, 256), F32),
            pltpu.VMEM((2 * rows, 128), F32),
            pltpu.VMEM((rows, 256), F32),
            pltpu.VMEM((rows, 128), F32),
            pltpu.VMEM((tok, 128), F32),
            pltpu.VMEM((tok, 128), F32),
            pltpu.VMEM((4, tok // 4, d), BF16),
            pltpu.VMEM(queries.shape, BF16),
            pltpu.VMEM(keys_raw.shape, BF16),
            pltpu.VMEM((1, 128), F32),
            pltpu.VMEM((1, 128), F32),
            pltpu.VMEM((4, 2, 256, d), BF16),
            pltpu.VMEM((1, d), F32),
            pltpu.VMEM((3 * NZ * NX * 2, 32, units), BF16),
            pltpu.VMEM((4, tok, width), BF16),
            pltpu.VMEM((tok, d), F32),
            pltpu.VMEM((4, tok // 4, d), BF16),
            pltpu.VMEM((tok, d), BF16),
            pltpu.VMEM((2, tok, units), F32),
            pltpu.VMEM((tok, units), BF16),
            pltpu.VMEM((NZ, 4, tok // 4, 256), BF16),
            pltpu.VMEM((NZ, 2, tok // 8, 256), BF16),
            pltpu.VMEM((NZ, 6, tok // 8, 256), BF16),
            pltpu.VMEM((tok // 4, d), BF16),
            dma((11,)),
            dma,
            dma((N_SLOTS,)),
            dma,
            dma((3,)),
            dma((3,)),
            dma((3, NZ * NX)),
            dma,
            dma((3, NZ)),
            dma,
            dma((3, 6)),
            dma((3,)),
            dma,
            dma,
            dma((NZ, 2)),
            dma,
            dma,
        ],
        compiler_params=pltpu.CompilerParams(
            collective_id=0, has_side_effects=True, vmem_limit_bytes=60 * 2**20
        ),
    )(
        residual_in, queries, keys_raw, values_raw.reshape(2, 128, 128), query_gain[None], key_gain[None],
        out_weight.reshape(2, 256, d),
        norm_gain[None], gate_weight, up_weight, down_weight.T,
    )


def solution(mesh):
    placed = (
        P(("sp", "tp"), None),
        P("sp", "tp"),
        P("sp", "tp"),
        P("sp", "tp"),
        P(),
        P(),
        P("tp", None),
        P(),
        P("sp", "tp"),
        P("sp", "tp"),
        P("tp", "sp"),
    )
    return jax.shard_map(
        per_device, mesh=mesh, in_specs=placed, out_specs=P(("sp", "tp"), None), check_vma=False
    )
```

```python
import math

import jax
import jax.numpy as jnp
from jax import lax
from jax.experimental import pallas as pl
from jax.experimental.pallas import tpu as pltpu
from jax.sharding import PartitionSpec as P

GRID_W = 64
EPS = 1e-06
THETA = 10000.0
MESH = pl.DeviceIdType.MESH
NZ, NX = 8, 4
F32 = jnp.float32
BF16 = jnp.bfloat16


MIRROR = {"z+": "z-", "z-": "z+", "x+": "x-", "x-": "x+"}


def next_hops(color, dz, dx):
    if color >= 2:
        return [(MIRROR[link], -a, -b) for link, a, b in next_hops(color - 2, -dz, -dx)]
    out = []
    if color == 0:
        if dx == 0:
            if 0 <= dz < 4:
                out.append(("z+", dz + 1, 0))
            if -3 < dz <= 0:
                out.append(("z-", dz - 1, 0))
            out.append(("x+", dz, 1))
            out.append(("x-", dz, -1))
        elif dx == 1 and dz % 2 == 0:
            out.append(("x+", dz, 2))
        elif dx == -1 and dz % 2 == 1:
            out.append(("x-", dz, -2))
    else:
        if dz == 0:
            if dx == 0:
                out.append(("x+", 0, 1))
                out.append(("x-", 0, -1))
            elif dx == 1:
                out.append(("x+", 0, 2))
            out.append(("z+", 1, dx))
            out.append(("z-", -1, dx))
        elif dz > 0:
            if dz < (4 if dx % 2 == 0 else 3):
                out.append(("z+", dz + 1, dx))
        else:
            if -dz < (3 if dx % 2 == 0 else 4):
                out.append(("z-", dz - 1, dx))
    return out


def blocks_of(color):
    seen, todo = [], [(0, 0)]
    while todo:
        at = todo.pop(0)
        seen.append(at)
        todo += [(dz, dx) for _, dz, dx in next_hops(color, *at)]
    assert len(seen) == NZ * NX and len({(dz % NZ, dx % NX) for dz, dx in seen}) == NZ * NX
    return seen


W_COLOR = (3, 0, 2)
GU_PLANES = (0, -1, 1, -2, 2, -3, 3, 4)
DOWN_PLANES = (0, 1, -1, 2, -2, 3, -3, 4)
LAG = 7
SCHEDULE = {
    'start': [
        (3, 0, 0), (4, 0, 0),
    ],
    'chunk0': [
        (0, 0, 0), (1, 0, 0), (2, 0, 0), (3, 1, 0), (3, 0, 1), (3, 0, -1), (3, -1, 0), (4, 1, 0), (4, -1, 0),
        (5, 0, 0), (4, 0, -1), (5, 1, 0), (4, 0, 1),
    ],
    'chunk1': [
        (1, 0, -1), (0, 1, 0), (1, 0, 1), (0, -1, 0), (2, 0, 1), (2, 0, -1), (3, 2, 0), (3, 1, 1), (3, -2, 0),
        (3, 1, -1), (4, 2, 0), (3, 0, 2), (3, -1, -1), (4, -2, 0),
    ],
    'chunk2': [
        (4, 1, -1), (4, -1, -1), (4, 0, 2), (4, -1, 1), (4, 1, 1), (3, -1, 1), (2, 0, -2),
    ],
    'chunk3': [
        (5, 2, 0), (5, 3, 0), (3, 2, -1), (3, -3, 0), (3, 2, 1), (3, -2, -1), (3, 1, -2), (3, 3, 0),
        (0, -2, 0), (1, 0, 2), (1, 1, 0), (4, 3, 0), (3, -2, 1), (3, -1, -2), (4, -3, 0),
    ],
    'chunk4': [
        (3, -3, -1), (4, 1, 2), (3, -3, 1), (4, 2, -1), (4, -2, -1), (4, -1, 2), (1, -1, 0),
    ],
    'chunk5': [
        (3, 2, 2), (3, 3, 1), (3, 3, -1), (4, 2, 1), (4, -2, 1), (3, 4, 0), (1, 1, -1), (0, -3, 0), (1, 1, 1),
        (3, -3, -2), (0, 2, 0), (4, -3, -1),
    ],
    'chunk6': [
        (3, -2, 2), (4, -2, 2), (4, 2, 2), (3, 3, -2), (4, 4, 0), (1, 2, 0), (1, -1, -1), (1, -1, 1),
        (1, -2, 0), (3, 4, 1), (3, 4, -1), (4, 3, -1),
    ],
    'chunk7': [
        (4, 3, 1), (4, -3, 1), (0, 0, -1), (0, -4, 0), (1, 1, -2), (1, 2, 1), (0, 3, 0), (2, 1, 0),
        (1, 2, -1), (4, -4, -1), (4, 3, 2), (1, -2, 1), (4, -3, 2), (1, -1, -2), (0, 0, 1), (3, 4, 2),
        (2, -1, 0), (1, -2, -1), (1, -3, 0), (1, 2, 2), (0, 1, -1), (4, -4, 1), (0, 0, -2), (2, 1, 1),
        (0, -1, -1), (2, 1, -1), (1, 3, 0), (4, 4, 2), (2, 2, 0), (1, -2, 2),
    ],
    'chunk8': [
        (0, -1, 1), (0, 1, 1), (2, -1, -1), (2, -2, 0), (2, -1, 1),
    ],
    'att': [
        (1, -3, 1), (0, 2, -1), (1, -3, -1), (1, 3, -1), (0, -1, -2),
    ],
    'own': [
        (0, 1, -2), (2, 1, 2), (0, -2, -1), (2, 2, -1), (1, 4, 0), (1, 3, 1), (0, -2, 1), (2, -2, -1),
        (2, 2, 1),
    ],
    'relay': [
        (2, 3, 0), (1, -3, -2), (0, 2, 1), (2, -2, 1), (0, -2, -2), (2, -3, 0),
    ],
    'two': [
        (1, 3, -2), (0, -3, -1), (0, 3, -1), (2, -1, 2), (2, 2, -2), (0, 2, -2), (1, 4, 1),
    ],
    'opp': [
        (0, -3, 1), (1, 4, -1),
    ],
    'k1': [
        (0, 3, 1), (0, -3, -2), (2, 3, 1),
    ],
    'k3': [
        (2, -2, -2), (0, 4, -1), (2, -3, 1),
    ],
    'k4': [
        (2, -4, 0),
    ],
    'k6': [
        (0, 3, -2), (2, 3, -1), (1, 4, 2), (0, -4, -2),
    ],
    'k7': [
        (2, -3, -1), (0, 4, 1), (2, 3, 2),
    ],
    'k8': [
        (2, -4, -1), (2, -3, 2),
    ],
    'plane3': [
        (2, -4, 1),
    ],
    'plane6': [
        (2, -4, -2),
    ],
}
SLOTS = [(what - 3, dz, dx) for events in SCHEDULE.values() for what, dz, dx in events if what in (3, 4)]
SLOT_OF = {b: i for i, b in enumerate(SLOTS)}
N_SLOTS = len(SLOTS)
PER = 8
BLOCK = 128


W_INDEX = [{b: i for i, b in enumerate(blocks_of(color))} for color in W_COLOR]


def rope(v, gain, cos, sin, lane):
    v = v * lax.rsqrt(jnp.mean(v * v, axis=-1, keepdims=True) + EPS) * gain
    turned = jnp.where(lane % 64 < 32, -pltpu.roll(v, 96, 1), pltpu.roll(v, 32, 1))
    return (v * cos + turned * sin).astype(BF16)


def layer_kernel(
    res_in, q_in, k_in, v_in, qg_in, kg_in, wo_in, ng_in, gate_in, up_in, down_in, out_hbm,
    kv, qall, acc, top, far_acc, far_top, cos_ref, sin_ref,
    res_ref, q_ref, k_ref, qg_ref, kg_ref, wo_ref, ng_ref,
    wbuf, att, proj, mix, rows_ref, gu_ref, hidden, terms, sums, parts, out_ref,
    in_sem, out_sem, kv_recv, kv_send, swap_recv, swap_send,
    w_recv, w_send, d2d_recv, d2d_send, ring_recv, ring_send, wo_recv, wo_send, rs_recv, rs_last, rs_send,
):
    me = lax.axis_index("sp")
    y = lax.axis_index("tp")
    core = me % 2
    chip = me // 2
    x = chip % NX
    z = chip // NX
    zs = {d: (z + NZ - d) % NZ for d in range(-4, 5)}
    xs = {d: (x + NX - d) % NX for d in range(-2, 3)}
    at = {
        "z+": (zs[-1] * NX + x) * 2 + core,
        "z-": (zs[1] * NX + x) * 2 + core,
        "x+": (z * NX + xs[-1]) * 2 + core,
        "x-": (z * NX + xs[1]) * 2 + core,
    }
    partner = chip * 2 + 1 - core
    y_up, y_down, y_far = (y + 1) % 4, (y + 3) % 4, (y + 2) % 4
    barrier = pltpu.get_barrier_semaphore()
    for dev in (*at.values(), partner):
        pl.semaphore_signal(barrier, inc=1, device_id={"sp": dev}, device_id_type=MESH)
    for dev in (y_up, y_down):
        pl.semaphore_signal(barrier, inc=1, device_id={"tp": dev}, device_id_type=MESH)

    pairs = [(k_in, k_ref), (kg_in, kg_ref), (v_in, kv.at[pl.ds(0, 2), :, pl.ds(128, 128)])]
    pairs += [(q_in, q_ref), (qg_in, qg_ref)]
    pairs += [(res_in, res_ref.at[y])]
    pairs += [(wo_in, wo_ref.at[0])]
    pairs += [(w, wbuf.at[2 * (NZ * NX * m + z * NX + x) + core]) for m, w in enumerate((gate_in, up_in, down_in))]
    pairs += [(ng_in, ng_ref)]
    loads = [pltpu.make_async_copy(a, b, in_sem.at[i]) for i, (a, b) in enumerate(pairs)]
    for load in loads:
        load.start()

    tok = q_ref.shape[0]
    heads = q_ref.shape[1] // 128
    rows = heads * tok
    scale = math.log2(math.e) / math.sqrt(128)
    lane = lax.broadcasted_iota(jnp.int32, (tok, 128), 1)
    token = lax.broadcasted_iota(jnp.int32, (tok, 128), 0) + me * tok
    place = jnp.where(lane < 64, token // GRID_W, token % GRID_W).astype(F32)
    angle = place * jnp.exp2((lane % 32).astype(F32) * (-math.log2(THETA) / 32))
    cos_ref[...] = jnp.cos(angle)
    sin_ref[...] = jnp.sin(angle)
    for load in loads[:3]:
        load.wait()
    k_rot = rope(k_ref[...].astype(F32), kg_ref[...], cos_ref[...], sin_ref[...], lane)
    for h in (0, 1):
        kv[h, :, 0:128] = k_rot[h * 128 : (h + 1) * 128]
    pl.semaphore_wait(barrier, 7)

    def send_on(slot):
        color, dz, dx = SLOTS[slot]
        for link, dz2, dx2 in next_hops(color, dz, dx):
            to = SLOT_OF[(color, dz2, dx2)]
            pltpu.make_async_remote_copy(
                kv.at[slot], kv.at[to], kv_send, kv_recv.at[to],
                device_id={"sp": at[link]}, device_id_type=MESH,
            ).start()

    def arrived(slot):
        pltpu.make_async_remote_copy(
            kv.at[slot], kv.at[slot], kv_send, kv_recv.at[slot],
            device_id={"sp": partner}, device_id_type=MESH,
        ).wait_recv()

    def gather_y(n, ref, own, below, above, slot_up, slot_down, far_up, far_down, piece):
        def hop(i, src, dst, k, dev):
            return pltpu.make_async_remote_copy(
                ref.at[src, *piece(k)], ref.at[dst, *piece(k)], ring_send.at[n], ring_recv.at[n, i],
                device_id={"tp": dev}, device_id_type=MESH,
            )

        return (
            [hop(k, own, slot_up, k, y_up) for k in (0, 1)],
            [hop(2 + k, own, slot_down, k, y_down) for k in (0, 1)],
            hop(4, below, far_up, 0, y_up),
            hop(5, above, far_down, 1, y_down),
        )

    def begin(ring):
        ups, downs, _, _ = ring
        ups[0].start()
        downs[1].start()
        ups[1].start()
        downs[0].start()

    res_ring = gather_y(0, res_ref, y, y_down, y_up, y, y, y_down, y_up, lambda k: (pl.ds(32 * k, 32),))
    wo_ring = gather_y(1, wo_ref, 0, 1, 2, 1, 2, 3, 3, lambda k: (core, pl.ds(128 * k, 128)))
    att_ring = gather_y(2, att, 0, 1, 2, 1, 2, 3, 3, lambda k: (pl.ds(128 * k, 128),))

    def wo_to_partner(slot, k):
        piece = wo_ref.at[slot, core, pl.ds(128 * k, 128)]
        pltpu.make_async_remote_copy(
            piece, piece, wo_send, wo_recv, device_id={"sp": partner}, device_id_type=MESH
        ).start()

    def pass_round(code):
        ring = (res_ring, wo_ring)[code // 2]
        if code % 2 == 0:
            ring[0][0].wait_recv()
            ring[2].start()
        else:
            ring[1][1].wait_recv()
            ring[3].start()
        if code >= 2:
            wo_to_partner(1 + code % 2, code % 2)

    send_on(0)
    send_on(1)
    for load in loads[5:7]:
        load.wait()
    begin(res_ring)
    begin(wo_ring)
    for load in loads[3:5]:
        load.wait()
    for h in range(heads):
        q_rot = rope(
            q_ref[:, h * 128 : (h + 1) * 128].astype(F32), qg_ref[...], cos_ref[...], sin_ref[...], lane
        )
        qall[rows + h * tok : rows + (h + 1) * tok, :] = q_rot

    def to_partner(src, dst, i):
        return pltpu.make_async_remote_copy(
            src, dst, swap_send.at[i], swap_recv.at[i], device_id={"sp": partner}, device_id_type=MESH
        )

    swap_q = to_partner(qall.at[pl.ds(rows, rows)], qall.at[pl.ds(0, rows)], 0)
    swap_acc = to_partner(acc.at[pl.ds(0, rows)], far_acc, 1)
    swap_top = to_partner(top.at[pl.ds(0, rows)], far_top, 2)
    swap_q.start()
    acc[...] = jnp.zeros_like(acc)
    top[...] = jnp.full_like(top, -1e30)
    for load in loads[7:]:
        load.wait()

    def weight_block(m, dz, dx):
        color = W_COLOR[m]
        block = wbuf.at[2 * (NZ * NX * m + zs[dz] * NX + xs[dx]) + core]
        n = W_INDEX[m][(dz, dx)]
        if (dz, dx) != (0, 0):
            pltpu.make_async_remote_copy(
                block, block, w_send, w_recv.at[m, n], device_id={"sp": partner}, device_id_type=MESH
            ).wait_recv()
        for link, dz2, dx2 in next_hops(color, dz, dx):
            pltpu.make_async_remote_copy(
                block, block, w_send, w_recv.at[m, W_INDEX[m][(dz2, dx2)]],
                device_id={"sp": at[link]}, device_id_type=MESH,
            ).start()
        pltpu.make_async_remote_copy(
            block, block, d2d_send, d2d_recv.at[m, dz % NZ], device_id={"sp": partner}, device_id_type=MESH
        ).start()

    def events(point):
        for what, dz, dx in SCHEDULE.get(point, ()):
            if what == 5:
                pass_round(dz)
            elif what >= 3:
                slot = SLOT_OF[(what - 3, dz, dx)]
                if slot >= 2:
                    arrived(slot)
                    send_on(slot)
            else:
                weight_block(what, dz, dx)

    def attend(first, blocks):
        keys = kv[pl.ds(first, PER), :, 0:128].reshape(PER * 128, 128)
        vals = kv[pl.ds(first, PER), :, 128:256].reshape(PER * 128, 128)
        wide = jnp.concatenate([vals, jnp.ones((PER * 128, 128), BF16)], axis=1)
        for i in blocks:
            r = slice(i * BLOCK, (i + 1) * BLOCK)
            s = lax.dot_general(qall[r, :], keys, (((1,), (1,)), ((), ())), preferred_element_type=F32)
            old = top[r, :]
            new = jnp.maximum(old, jnp.max(s, axis=1, keepdims=True))
            top[r, :] = new
            shrink = jnp.exp2((old - new) * scale)
            w = jnp.exp2(s * scale - new[:, 0:1] * scale).astype(BF16)
            o = jnp.dot(w, wide, preferred_element_type=F32)
            acc[r, 0:128] = acc[r, 0:128] * shrink + o[:, 0:128]
            acc[r, 128:256] = acc[r, 128:256] * shrink + o[:, 128:256]

    last = N_SLOTS // PER - 1

    def chunk(c, _):
        for k in range(1, N_SLOTS // PER - 1):

            @pl.when(c == k)
            def _():
                events(f"chunk{k}")
                if k == last - 1:
                    wo_ring[0][1].wait_recv()
                    wo_to_partner(1, 1)
                    wo_ring[1][0].wait_recv()
                    wo_to_partner(2, 0)

        attend(c * PER, range(2 * rows // BLOCK))
        return 0

    events("chunk0")
    swap_q.wait_recv()
    lax.fori_loop(0, last, chunk, 0)
    events(f"chunk{last}")
    attend(last * PER, range(rows // BLOCK))
    swap_acc.start()
    swap_top.start()
    attend(last * PER, range(rows // BLOCK, 2 * rows // BLOCK))
    events(f"chunk{last + 1}")
    for k in (0, 1):
        wo_ring[2 + k].wait_recv()
        wo_to_partner(3, k)
    swap_acc.wait_recv()
    swap_top.wait_recv()
    for h in range(heads):
        mine = pl.ds(rows + h * tok, tok)
        far = pl.ds(h * tok, tok)
        t1, t2 = top[mine, :], far_top[far, :]
        t = jnp.maximum(t1, t2)
        a1, a2 = jnp.exp2((t1 - t) * scale), jnp.exp2((t2 - t) * scale)
        num = acc[mine, 0:128] * a1 + far_acc[far, 0:128] * a2
        den = acc[mine, 128:256] * a1 + far_acc[far, 128:256] * a2
        att[0, :, h * 128 : (h + 1) * 128] = (num / den).astype(BF16)

    def group_term(g):
        term = jnp.dot(att[g], wo_ref[g].reshape(2 * tok, NZ * NX * 64), preferred_element_type=F32)
        return term.astype(BF16).astype(F32)

    begin(att_ring)
    events("att")
    proj[...] = group_term(0)
    events("own")
    att_ring[0][0].wait_recv()
    att_ring[2].start()
    att_ring[1][1].wait_recv()
    att_ring[3].start()
    events("relay")
    shared = wo_ref.at[pl.ds(1, 3), 1 - core]
    from_other = pltpu.make_async_remote_copy(
        shared, shared, wo_send, wo_recv, device_id={"sp": partner}, device_id_type=MESH
    )
    from_other.wait_recv()
    att_ring[0][1].wait_recv()
    proj[...] += group_term(1)
    att_ring[1][0].wait_recv()
    proj[...] += group_term(2)
    events("two")
    for c in (res_ring[0][0], res_ring[0][1], res_ring[1][0], res_ring[1][1], res_ring[2], res_ring[3]):
        if c is not res_ring[0][0] and c is not res_ring[1][1]:
            c.wait_recv()
    att_ring[2].wait_recv()
    att_ring[3].wait_recv()
    proj[...] += group_term(3)
    for j in range(4):
        r = slice(64 * j, 64 * (j + 1))
        mixed = (res_ref[j].astype(F32) + proj[r]).astype(BF16)
        mix[j] = mixed
        mixed_f = mixed.astype(F32)
        normed = mixed_f * lax.rsqrt(jnp.mean(mixed_f * mixed_f, axis=-1, keepdims=True) + EPS) * ng_ref[...]
        rows_ref[r] = normed.astype(BF16)
    events("opp")

    def plane_of(m, dz):
        four = wbuf.at[pl.ds(0, NX)]
        pltpu.make_async_remote_copy(
            four, four, d2d_send, d2d_recv.at[m, dz % NZ], device_id={"sp": partner}, device_id_type=MESH
        ).wait_recv()
        return wbuf[pl.ds(2 * (NZ * NX * m + NX * zs[dz]), 2 * NX)].reshape(64 * NX, units)

    units = hidden.shape[1]
    for n, dz in enumerate(GU_PLANES):
        lhs = rows_ref[:, pl.ds(pl.multiple_of(256 * zs[dz], 256), 256)]
        for m in (0, 1):
            part = jnp.dot(lhs, plane_of(m, dz), preferred_element_type=F32)
            gu_ref[m] = part if n == 0 else gu_ref[m] + part
        events(f"k{n + 1}")
    gate = gu_ref[0]
    hidden[...] = (gate / (1.0 + jnp.exp(-gate)) * gu_ref[1]).astype(BF16)

    def plane_copies(i):
        def hop(n, src, dev):
            return pltpu.make_async_remote_copy(
                src, parts.at[i, n], rs_send, rs_recv.at[i, n] if n < 2 else rs_last,
                device_id={"tp": dev}, device_id_type=MESH,
            )

        low, high = pl.ds(0, 32), pl.ds(32, 32)
        return [
            hop(0, terms.at[i, y_far, low], y_up),
            hop(1, terms.at[i, y_far, high], y_down),
            hop(2, terms.at[i, y_up, high], y_up),
            hop(3, terms.at[i, y_down, low], y_down),
            hop(4, sums.at[i, 0], y_up),
            hop(5, sums.at[i, 1], y_down),
        ]

    copies = [plane_copies(i) for i in range(NZ)]

    def add_and_pass(i):
        copies[i][0].wait_recv()
        sums[i, 0] = (parts[i, 0].astype(F32) + terms[i, y_up, 0:32].astype(F32)).astype(BF16)
        copies[i][4].start()
        copies[i][1].wait_recv()
        sums[i, 1] = (parts[i, 1].astype(F32) + terms[i, y_down, 32:64].astype(F32)).astype(BF16)
        copies[i][5].start()

    for i, dz in enumerate(DOWN_PLANES):
        piece = lax.dot_general(hidden[...], plane_of(2, dz), (((1,), (1,)), ((), ())), preferred_element_type=F32)
        terms[i] = piece.astype(BF16).reshape(4, 64, 256)
        for c in copies[i][:4]:
            c.start()
        events(f"plane{i}")
        if i >= LAG:
            add_and_pass(i - LAG)
    for i in range(NZ - LAG, NZ):
        add_and_pass(i)
    last_pieces = parts.at[:, pl.ds(2, 4)]
    pltpu.make_async_remote_copy(
        last_pieces, last_pieces, rs_send, rs_last, device_id={"tp": y_up}, device_id_type=MESH
    ).wait_recv()
    for i, dz in enumerate(DOWN_PLANES):
        cols = pl.ds(pl.multiple_of(256 * zs[dz], 256), 256)
        for h, (a, b) in enumerate(((3, 4), (2, 5))):
            r = slice(32 * h, 32 * (h + 1))
            fed = terms[i, y, r].astype(F32) + parts[i, a].astype(F32) + parts[i, b].astype(F32)
            out_ref[r, cols] = (mix[y, r, cols].astype(F32) + 0.5 * fed).astype(BF16)
    out = pltpu.make_async_copy(out_ref, out_hbm, out_sem)
    out.start()
    moved = kv.at[pl.ds(0, N_SLOTS - 2)]
    pltpu.make_async_remote_copy(
        moved, moved, kv_send, kv_recv.at[0], device_id={"sp": partner}, device_id_type=MESH
    ).wait_send()
    for blocks, sem in ((3 * (NZ * NX - 1), w_send), (3 * NZ * NX, d2d_send)):
        moved = wbuf.at[pl.ds(0, blocks)]
        pltpu.make_async_remote_copy(
            moved, moved, sem, d2d_recv.at[0, 0], device_id={"sp": partner}, device_id_type=MESH
        ).wait_send()
    for n, sent in enumerate((res_ref.at[pl.ds(0, 3)], wo_ref.at[pl.ds(0, 3), 0], att.at[pl.ds(0, 3)])):
        pltpu.make_async_remote_copy(
            sent, sent, ring_send.at[n], ring_recv.at[n, 0], device_id={"tp": y_up}, device_id_type=MESH
        ).wait_send()
    for c in (swap_q, swap_acc, swap_top, from_other):
        c.wait_send()
    pltpu.make_async_remote_copy(
        parts, parts, rs_send, rs_last, device_id={"tp": y_up}, device_id_type=MESH
    ).wait_send()
    out.wait()


def per_device(
    residual_in,
    queries,
    keys_raw,
    values_raw,
    query_gain,
    key_gain,
    out_weight,
    norm_gain,
    gate_weight,
    up_weight,
    down_weight,
):
    tok, width = queries.shape
    rows = tok * width // 128
    d = residual_in.shape[1]
    units = gate_weight.shape[1]
    dma = pltpu.SemaphoreType.DMA
    return pl.pallas_call(
        layer_kernel,
        out_shape=jax.ShapeDtypeStruct(residual_in.shape, BF16),
        in_specs=[pl.BlockSpec(memory_space=pl.ANY)] * 11,
        out_specs=pl.BlockSpec(memory_space=pl.ANY),
        scratch_shapes=[
            pltpu.VMEM((N_SLOTS, 128, 256), BF16),
            pltpu.VMEM((2 * rows, 128), BF16),
            pltpu.VMEM((2 * rows, 256), F32),
            pltpu.VMEM((2 * rows, 128), F32),
            pltpu.VMEM((rows, 256), F32),
            pltpu.VMEM((rows, 128), F32),
            pltpu.VMEM((tok, 128), F32),
            pltpu.VMEM((tok, 128), F32),
            pltpu.VMEM((4, tok // 4, d), BF16),
            pltpu.VMEM(queries.shape, BF16),
            pltpu.VMEM(keys_raw.shape, BF16),
            pltpu.VMEM((1, 128), F32),
            pltpu.VMEM((1, 128), F32),
            pltpu.VMEM((4, 2, 256, d), BF16),
            pltpu.VMEM((1, d), F32),
            pltpu.VMEM((3 * NZ * NX * 2, 32, units), BF16),
            pltpu.VMEM((4, tok, width), BF16),
            pltpu.VMEM((tok, d), F32),
            pltpu.VMEM((4, tok // 4, d), BF16),
            pltpu.VMEM((tok, d), BF16),
            pltpu.VMEM((2, tok, units), F32),
            pltpu.VMEM((tok, units), BF16),
            pltpu.VMEM((NZ, 4, tok // 4, 256), BF16),
            pltpu.VMEM((NZ, 2, tok // 8, 256), BF16),
            pltpu.VMEM((NZ, 6, tok // 8, 256), BF16),
            pltpu.VMEM((tok // 4, d), BF16),
            dma((11,)),
            dma,
            dma((N_SLOTS,)),
            dma,
            dma((3,)),
            dma((3,)),
            dma((3, NZ * NX)),
            dma,
            dma((3, NZ)),
            dma,
            dma((3, 6)),
            dma((3,)),
            dma,
            dma,
            dma((NZ, 2)),
            dma,
            dma,
        ],
        compiler_params=pltpu.CompilerParams(
            collective_id=0, has_side_effects=True, vmem_limit_bytes=60 * 2**20
        ),
    )(
        residual_in, queries, keys_raw, values_raw.reshape(2, 128, 128), query_gain[None], key_gain[None],
        out_weight.reshape(2, 256, d),
        norm_gain[None], gate_weight, up_weight, down_weight.T,
    )


def solution(mesh):
    placed = (
        P(("sp", "tp"), None),
        P("sp", "tp"),
        P("sp", "tp"),
        P("sp", "tp"),
        P(),
        P(),
        P("tp", None),
        P(),
        P("sp", "tp"),
        P("sp", "tp"),
        P("tp", "sp"),
    )
    return jax.shard_map(
        per_device, mesh=mesh, in_specs=placed, out_specs=P(("sp", "tp"), None), check_vma=False
    )
```
